32 devices in a mesh: sp: 8 (over z, y), tp: 4 (over x, core).
Axes of the slice: x: 2, y: 2, z: 4, core: 2. Of those that a mesh axis runs over, the one named last changes fastest.
Arguments:
- mixer_output_stream: bfloat16 [1024, 2048], P('sp', 'tp'), may hold values from -6 to 6
- layer_output_gradient: bfloat16 [1024, 2048], P('sp', 'tp'), may hold values from -2.5 to 2.5
- routes: int32 [1024, 2], P('sp'), may hold values from 0 to 7, all different within a row; in each aligned block of 128 rows (0 to 127, 128 to 255, ...) at most 48 rows name the same one
- expert_combine_weight: float32 [1024, 2], P('sp'), may hold values from 0.2 to 1
- expert_gate_weight: bfloat16 [8, 2048, 3584], P('sp', None, 'tp'), may hold values from -0.125 to 0.125
- expert_up_weight: bfloat16 [8, 2048, 3584], P('sp', None, 'tp'), may hold values from -0.125 to 0.125
- expert_down_weight: bfloat16 [8, 3584, 2048], P('sp', 'tp'), may hold values from -0.09375 to 0.09375
- head_mixer_input: bfloat16 [1024, 4096], P('sp', 'tp'), may hold values from -6 to 6
- head_step_size: float32 [1024, 64], P('sp', 'tp'), may hold values from 0.25 to 4
- head_decay_rate: float32 [64], P('tp'), may hold values from 0 to 1
- extra_log_decay: float32 [1024, 64], P('sp', 'tp'), may hold values from -3 to 0
- state_entering_span: float32 [64, 64, 128], P('tp'), may hold values from -48 to 48
- state_input_vectors: bfloat16 [1024, 1024], P('sp', 'tp'), may hold values from -1.75 to 1.75
- state_readout_vectors: bfloat16 [1024, 1024], P('sp', 'tp'), may hold values from -1.75 to 1.75
- gate_preactivation: bfloat16 [1024, 4096], P('sp', 'tp'), may hold values from -6 to 6
- group_norm_scale: float32 [4096], P('tp'), may hold values from 0.1 to 1.9
- mixer_output_weight: bfloat16 [4096, 2048], P('tp', 'sp'), may hold values from -0.09375 to 0.09375
Outputs:
- grad_gate: bfloat16 [8, 2048, 3584], P('sp', None, 'tp')
- grad_up: bfloat16 [8, 2048, 3584], P('sp', None, 'tp')
- grad_down: bfloat16 [8, 3584, 2048], P('sp', 'tp')
- grad_out_proj: float32 [4096, 2048], P('tp', 'sp')
- grad_input: bfloat16 [1024, 4096], P('sp', 'tp')
- grad_step: float32 [1024, 64], P('sp', 'tp')
- grad_state_in: bfloat16 [1024, 1024], P('sp', 'tp')
- grad_read_out: bfloat16 [1024, 1024], P('sp', 'tp')
- grad_gate_in: bfloat16 [1024, 4096], P('sp', 'tp')
The draws below stay inside these ranges and needn't reach their ends.
Inputs may be any that keep to these rules, and one draw needn't show every extreme that they name: `routes`: the two experts of a token differ. In each aligned block of 128 rows no expert is named more than 48 times, and in every draw some expert is named exactly 48 times in some block.
All inputs are finite; a program needn't handle non-finite values.
Results may differ from the reference program's by a relative error of at most 0.02.
Values may be sent and summed in bfloat16 or wider, within the bound.
A program may use at most 128 MiB of HBM per device.

```python
import math
from functools import partial
import jax
import jax.numpy as jnp
import numpy as np
from jax import lax

D = 2048
FF = 3584
HEADS = 64
HDIM = 64
GROUPS = 8
STATE = 128
BLK = 128
TOP = 2
TOK_DEV = 128
DI = 4096
EXPERTS = 8
CAP = 48
TOKENS = 1024
N_TP = 4


def draw_head_step_size(key, part):
    first, second = jax.random.split(key)
    rough = jnp.exp(jax.random.uniform(first, (TOKENS, HEADS), jnp.float32, math.log(0.5), math.log(2.0)))
    spans = TOKENS // TOK_DEV
    factor = jnp.exp(jax.random.uniform(second, (spans, 1, 1), jnp.float32, math.log(0.5), math.log(2.0)))
    return (rough.reshape(spans, TOK_DEV, HEADS) * factor).reshape(TOKENS, HEADS)


def draw_head_decay_rate(key, part):
    first, second = jax.random.split(key)
    picks = jax.random.randint(first, (HEADS,), 0, 8)
    limit = 4
    spread = jnp.exp(jax.random.uniform(second, (HEADS,), jnp.float32, math.log(0.5), math.log(2.0)))
    fast_rate = 3.0 / BLK * spread
    slow_rate = 0.25 / TOKENS * spread
    return jnp.where(picks < limit, fast_rate, slow_rate)


def draw_extra_log_decay(key, part):
    first, second = jax.random.split(key)
    places = jax.random.randint(first, (3,), 0, TOKENS)
    amounts = jnp.log(jax.random.uniform(second, (3, HEADS), jnp.float32, 0.5, 0.8))
    hits = (jnp.arange(TOKENS, dtype=jnp.int32)[:, None] == places[None, :]).astype(jnp.float32)
    return jnp.dot(hits, amounts, precision=lax.Precision.HIGHEST)


def strengthened(result, rng, source, target, parts, factor):
    owner, partner = [(jnp.arange(result.shape[dim]) // (result.shape[dim] // parts)).reshape([-1 if axis == dim else 1 for axis in range(result.ndim)]) for dim in (source, target)]
    chosen = jax.random.permutation(rng, parts)[partner]
    strong = (owner == chosen) | (owner == (partner + parts // 2) % parts)
    return jnp.where(strong, factor * result, result)


def level_of(own_key, shape, cuts, smallest, high):
    factor_of, own = 1.0, jax.random.fold_in(own_key, 6)
    for dim, parts in cuts:
        steps = jnp.exp(jax.random.uniform(jax.random.fold_in(own, dim), (parts,), jnp.float32, smallest / len(cuts), high / len(cuts)))
        factor_of = factor_of * jnp.repeat(steps, shape[dim] // parts).reshape([-1 if axis == dim else 1 for axis in range(len(shape))])
    return factor_of


def deal_out(stream_key, own, number, rows, number_of, top, most, slope):
    ranking = jax.random.permutation(stream_key, number_of)
    heavy_load, common = portions_of(number_of, rows * top, most, slope, True), portions_of(number_of, rows * top, most, slope, False)
    places = jnp.arange(number_of)

    def named(sizes, turn):
        used = int((sizes > 0).sum())
        fixed = max(1, used // 4)
        moved = fixed + (places - fixed + turn * (used - fixed)) % max(1, number_of - fixed)
        return jnp.zeros((number_of,), jnp.int32).at[ranking[jnp.where(places < fixed, places, moved)]].set(jnp.asarray(sizes, jnp.int32))

    sizes = jnp.where(number % 4 == 0, named(heavy_load, number // 4), named(common, number - number // 4 - 1))
    mixed = jax.random.permutation(jax.random.fold_in(own, 3), number_of)
    source_of, receiver = mixed[0:number_of // 2 * 2:2], mixed[1:number_of // 2 * 2:2]
    room = jnp.minimum(sizes[source_of] - 1, most - sizes[receiver]) // 2
    room = jnp.where((source_of == ranking[0]) | (receiver == ranking[0]) | (sizes[receiver] == 0), 0, jnp.maximum(room, 0))
    moved = jax.random.randint(jax.random.fold_in(own, 4), (number_of // 2,), 0, 1 << 20) % (room + 1)
    sizes = sizes.at[source_of].add(-moved).at[receiver].add(moved)
    members = jnp.searchsorted(jnp.cumsum(sizes), jnp.arange(rows * top), side="right").astype(jnp.int32)
    table = members.reshape(top, rows).T
    table = table[jax.random.permutation(jax.random.fold_in(own, 1), rows)]
    turn = jax.random.randint(jax.random.fold_in(own, 2), (rows, 1), 0, top)
    return jnp.take_along_axis(table, (jnp.arange(top)[None, :] + turn) % top, axis=1)


def portions_of(number_of, total, bound, slope, full):
    portions = [(1 << 20) // math.isqrt(rank ** slope) + 1 for rank in range(1, number_of + 1)]
    largest = bound if full else min(bound, max(-(-total // number_of), total * portions[0] // sum(portions)))
    least = 1 if total - largest >= number_of - 1 else 0
    counts, spare = [largest] + [least] * (number_of - 1), total - largest - least * (number_of - 1)
    while spare > 0:
        free = [i for i in range(1, number_of) if counts[i] < largest] or [i for i in range(1, number_of) if counts[i] < bound]
        mass, remaining = sum([portions[i] for i in free]), spare
        for i in free:
            addition = min(bound - counts[i], max(1, remaining * portions[i] // mass), spare)
            counts[i] = counts[i] + addition
            spare = spare - addition
    return np.array(counts)


def scatter_about(stream_key, extent, deviation, most, pieces=(), held_as=jnp.bfloat16):
    values = deviation * jax.random.normal(stream_key, extent, jnp.float32)
    if pieces:
        values = values * level_of(stream_key, extent, pieces, -0.22, 0.18)
    return jnp.clip(values, -most, most).astype(held_as)


def gaussian_with(key, shape, width, bound, shards, heavy, held_as=jnp.bfloat16):
    entries = width * jax.random.normal(key, shape, jnp.float32)
    if shards:
        entries = entries * level_of(key, shape, shards, -0.22, 0.18)
    return jnp.clip(strengthened(entries, jax.random.fold_in(key, 3), *heavy), -bound, bound).astype(held_as)


def setup_inputs(seed: int = 0) -> dict:
    seeds = jax.random.split(jax.random.key(seed), 18)
    mixer_output_stream = scatter_about(seeds[0], (TOKENS, D), 1.0, 6.0, ((0, 8), (1, 4)))
    layer_output_gradient = gaussian_with(seeds[1], (TOKENS, D), 0.3, 2.5, ((0, 8), (1, 4)), (0, 1, 8, 2.0))
    routes_keys = jax.random.split(jax.random.fold_in(seeds[2], 1), TOKENS // TOK_DEV)
    routes_turns = jax.random.permutation(jax.random.fold_in(seeds[2], 3), TOKENS // TOK_DEV)
    routes = jax.vmap(lambda own, number: deal_out(jax.random.fold_in(seeds[2], 2), own, number, TOK_DEV, EXPERTS, TOP, CAP, 1))(routes_keys, routes_turns).reshape((TOKENS, TOP))
    expert_combine_weight = jnp.clip(0.2 + 0.8 * jax.random.uniform(seeds[3], (TOKENS, TOP), jnp.float32) ** level_of(seeds[3], (TOKENS, TOP), ((0, 8),), -0.2, 0.2), 0.2, 1.0)
    expert_gate_weight = scatter_about(seeds[4], (EXPERTS, D, FF), D ** -0.5, 0.125, ((0, 8), (2, 4)))
    expert_up_weight = scatter_about(seeds[5], (EXPERTS, D, FF), D ** -0.5, 0.125, ((0, 8), (2, 4)))
    expert_down_weight = scatter_about(seeds[6], (EXPERTS, FF, D), FF ** -0.5, 0.09375, ((0, 8), (1, 4)))
    head_mixer_input = scatter_about(seeds[7], (TOKENS, DI), 1.0, 6.0, ((0, 8), (1, 4)))
    head_step_size = draw_head_step_size(jax.random.fold_in(seeds[17], 71), 0)
    head_decay_rate = draw_head_decay_rate(jax.random.fold_in(seeds[17], 71), 0)
    extra_log_decay = draw_extra_log_decay(jax.random.fold_in(seeds[17], 71), 0)
    state_entering_span = scatter_about(seeds[11], (HEADS, HDIM, STATE), 8.0, 48.0, ((0, 4),), jnp.float32)
    state_input_vectors = scatter_about(seeds[12], (TOKENS, GROUPS * STATE), (STATE ** -0.25), 1.75, ((0, 8), (1, 4)))
    state_readout_vectors = scatter_about(seeds[13], (TOKENS, GROUPS * STATE), (STATE ** -0.25), 1.75, ((0, 8), (1, 4)))
    gate_preactivation = scatter_about(seeds[14], (TOKENS, DI), 1.0, 6.0, ((0, 8), (1, 4)))
    group_norm_scale = jnp.clip(1.0 + 0.18 * jax.random.normal(seeds[15], (DI,), jnp.float32), 0.1, 1.9)
    mixer_output_weight = scatter_about(seeds[16], (DI, D), DI ** -0.5, 0.09375, ((0, 4), (1, 8)))
    return dict(mixer_output_stream=mixer_output_stream, layer_output_gradient=layer_output_gradient, routes=routes, expert_combine_weight=expert_combine_weight, expert_gate_weight=expert_gate_weight, expert_up_weight=expert_up_weight, expert_down_weight=expert_down_weight, head_mixer_input=head_mixer_input, head_step_size=head_step_size, head_decay_rate=head_decay_rate, extra_log_decay=extra_log_decay, state_entering_span=state_entering_span, state_input_vectors=state_input_vectors, state_readout_vectors=state_readout_vectors, gate_preactivation=gate_preactivation, group_norm_scale=group_norm_scale, mixer_output_weight=mixer_output_weight)


norm_eps = 1e-05
exact_mode = lax.Precision.HIGHEST

def span_local_scan(input_heads, time_step, decay_speed, sudden_decay, input_vector_groups, readout_groups, starting_state):
    length, head_count, head_size = input_heads.shape
    groups, state_size = (input_vector_groups.shape[1], input_vector_groups.shape[2])
    per_group = head_count // groups
    block_count = length // BLK
    log_decay_total = sudden_decay - time_step * decay_speed[None, :]
    scaled = (input_heads * time_step[:, :, None]).reshape(block_count, BLK, groups, per_group, head_size)
    log_decay_total = log_decay_total.reshape(block_count, BLK, groups, per_group)
    b_rows = input_vector_groups.reshape(block_count, BLK, groups, state_size)
    c_rows = readout_groups.reshape(block_count, BLK, groups, state_size)
    cumulative = jnp.cumsum(log_decay_total, axis=1)
    causal_mask = jnp.tril(jnp.ones((BLK, BLK), dtype=bool))
    cum_t = jnp.moveaxis(cumulative, 1, -1)
    gaps = cum_t[..., :, None] - cum_t[..., None, :]
    decays = jnp.where(causal_mask, jnp.exp(jnp.where(causal_mask, gaps, 0.0)), 0.0)
    affinity = jnp.einsum('blgn,bsgn->bgls', c_rows, b_rows, precision=exact_mode)
    y_diag = jnp.einsum('bghls,bsghp->blghp', affinity[:, :, None] * decays, scaled, precision=exact_mode)
    to_end = jnp.exp(cumulative[:, -1:] - cumulative)
    states = jnp.einsum('blgn,blghp->bghpn', b_rows, scaled * to_end[..., None], precision=exact_mode)
    block_decay = jnp.exp(cumulative[:, -1])

    def advance(running, inputs):
        block_state, decay_now = inputs
        return (decay_now[..., None, None] * running + block_state, running)
    first_state = starting_state.reshape(groups, per_group, head_size, state_size)
    closing_state, incoming_state = lax.scan(advance, first_state, (states, block_decay))
    y_off = jnp.einsum('blgn,bghpn->blghp', c_rows, incoming_state, precision=exact_mode) * jnp.exp(cumulative)[..., None]
    result_rows = (y_diag + y_off).reshape(length, head_count, head_size)
    return (result_rows, closing_state.reshape(head_count, head_size, state_size))

def gate_norm(scan_out, gate_vals, group_norm_scale, groups):
    length = scan_out.shape[0]
    gated = scan_out.reshape(length, -1) * jax.nn.silu(gate_vals)
    grouped = gated.reshape(length, groups, -1)
    factor = lax.rsqrt(lax.optimization_barrier(jnp.mean(grouped * grouped, axis=-1, keepdims=True)) + norm_eps)
    return (grouped * factor).reshape(length, -1) * group_norm_scale[None, :]

def slot_index(route_rows, expert_count, capacity):
    flat_routes = route_rows.reshape(-1)
    onehot = (flat_routes[:, None] == jnp.arange(expert_count, dtype=jnp.int32)[None, :]).astype(jnp.int32)
    before = jnp.cumsum(onehot, axis=0) - onehot
    return flat_routes * capacity + lax.optimization_barrier(jnp.sum(before * onehot, axis=1))

def build_table(destination, slot_count):
    pair_count = destination.shape[0]
    return jnp.full((slot_count,), pair_count, jnp.int32).at[destination].set(jnp.arange(pair_count, dtype=jnp.int32))

def pack_rows(stream, grad_rows, slot_table, weights):
    token_of = slot_table // 2
    routed = jnp.take(stream, token_of, axis=0, mode='fill', fill_value=0)
    weight_of = jnp.take(weights.reshape(-1), slot_table, mode='fill', fill_value=0.0)
    picked = jnp.take(grad_rows, token_of, axis=0, mode='fill', fill_value=0).astype(jnp.float32)
    return (routed, (picked * weight_of[:, None]).astype(jnp.bfloat16))

def expert_hidden(routed_rows, routed_grads, w_gate, w_up, w_down):
    pre_gate = jnp.dot(routed_rows, w_gate, preferred_element_type=jnp.float32)
    pre_up = jnp.dot(routed_rows, w_up, preferred_element_type=jnp.float32)
    activated = jax.nn.silu(pre_gate)
    hidden = (activated * pre_up).astype(jnp.bfloat16)
    hidden_grad = lax.dot_general(routed_grads, w_down, (((1,), (1,)), ((), ())), preferred_element_type=jnp.float32)
    sigmoid_gate = jax.nn.sigmoid(pre_gate)
    gate_grad = (hidden_grad * pre_up * sigmoid_gate * (1.0 + pre_gate * (1.0 - sigmoid_gate))).astype(jnp.bfloat16)
    up_grad = (hidden_grad * activated).astype(jnp.bfloat16)
    return (hidden, gate_grad, up_grad)

def expert_weight_grads(routed_rows, routed_grads, hidden, gate_grad, up_grad):
    contract = (((0,), (0,)), ((), ()))
    grad_g = lax.dot_general(routed_rows, gate_grad, contract, preferred_element_type=jnp.float32)
    grad_u = lax.dot_general(routed_rows, up_grad, contract, preferred_element_type=jnp.float32)
    grad_d = lax.dot_general(hidden, routed_grads, contract, preferred_element_type=jnp.float32)
    return (grad_g.astype(jnp.bfloat16), grad_u.astype(jnp.bfloat16), grad_d.astype(jnp.bfloat16))

def row_partial(gate_grad, up_grad, w_gate, w_up):
    contract = (((1,), (1,)), ((), ()))
    partial_sum = lax.dot_general(gate_grad, w_gate, contract, preferred_element_type=jnp.float32)
    partial_sum = partial_sum + lax.dot_general(up_grad, w_up, contract, preferred_element_type=jnp.float32)
    return lax.optimization_barrier(partial_sum.astype(jnp.bfloat16)).astype(jnp.float32)

def add_returns(grad_rows, returned, destination):
    token_count = grad_rows.shape[0]
    gathered = jnp.take(returned, destination, axis=0).reshape(token_count, -1, returned.shape[-1]).astype(jnp.float32)
    return (grad_rows.astype(jnp.float32) + lax.optimization_barrier(jnp.sum(gathered, axis=1))).astype(jnp.bfloat16)

def reference(mixer_output_stream, layer_output_gradient, routes, expert_combine_weight, expert_gate_weight, expert_up_weight, expert_down_weight, head_mixer_input, head_step_size, head_decay_rate, extra_log_decay, state_entering_span, state_input_vectors, state_readout_vectors, gate_preactivation, group_norm_scale, mixer_output_weight):
    blocks = TOKENS // TOK_DEV
    destination = jax.vmap(partial(slot_index, expert_count=EXPERTS, capacity=CAP))(routes.reshape(blocks, TOK_DEV, TOP))
    tables = jax.vmap(partial(build_table, slot_count=EXPERTS * CAP))(destination)
    sent_rows, sent_grads = jax.vmap(pack_rows)(mixer_output_stream.reshape(blocks, TOK_DEV, D), layer_output_gradient.reshape(blocks, TOK_DEV, D), tables, expert_combine_weight.reshape(blocks, TOK_DEV, TOP))

    def by_expert(values):
        return values.reshape(blocks, EXPERTS, CAP, D).transpose(1, 0, 2, 3).reshape(EXPERTS, blocks * CAP, D)

    def per_expert(packed):
        routed_rows, routed_grads, w_gate, w_up, w_down = packed
        hidden, gate_grad, up_grad = expert_hidden(routed_rows, routed_grads, w_gate, w_up, w_down)
        grad_g, grad_u, grad_d = expert_weight_grads(routed_rows, routed_grads, hidden, gate_grad, up_grad)
        block_width = w_gate.shape[1] // N_TP
        running = jnp.zeros((routed_rows.shape[0], w_gate.shape[0]), jnp.float32)
        for block_number in range(N_TP):
            first_col = block_number * block_width
            running = running + row_partial(gate_grad[:, first_col:first_col + block_width], up_grad[:, first_col:first_col + block_width], w_gate[:, first_col:first_col + block_width], w_up[:, first_col:first_col + block_width])
        return (grad_g, grad_u, grad_d, running.astype(jnp.bfloat16))
    grad_gate, grad_up, grad_down, returned = lax.map(per_expert, (by_expert(sent_rows), by_expert(sent_grads), expert_gate_weight, expert_up_weight, expert_down_weight))
    returned = returned.reshape(EXPERTS, blocks, CAP, D).transpose(1, 0, 2, 3).reshape(blocks, EXPERTS * CAP, D)
    mix_grad = jax.vmap(add_returns)(layer_output_gradient.reshape(blocks, TOK_DEV, D), returned, destination).reshape(TOKENS, D)
    input_heads = head_mixer_input.astype(jnp.float32).reshape(TOKENS, HEADS, HDIM)
    input_vector_groups = state_input_vectors.astype(jnp.float32).reshape(TOKENS, GROUPS, STATE)
    readout_groups = state_readout_vectors.astype(jnp.float32).reshape(TOKENS, GROUPS, STATE)

    def forward(input_values, time_step_values, input_vector_entries, readout_entries):
        result_rows, closing_state = span_local_scan(input_values, time_step_values, head_decay_rate, extra_log_decay, input_vector_entries, readout_entries, state_entering_span)
        return result_rows
    scan_out, pull_back = jax.vjp(forward, input_heads, head_step_size, input_vector_groups, readout_groups)

    def apply_norm(scan_vals, gate_vals):
        return gate_norm(scan_vals, gate_vals, group_norm_scale, GROUPS)
    normed, pull_norm = jax.vjp(apply_norm, scan_out, gate_preactivation.astype(jnp.float32))
    normed_low = normed.astype(jnp.bfloat16)
    grad_out_proj = lax.dot_general(normed_low, mix_grad, (((0,), (0,)), ((), ())), preferred_element_type=jnp.float32)
    normed_grad = lax.dot_general(mix_grad, mixer_output_weight, (((1,), (1,)), ((), ())), preferred_element_type=jnp.float32)
    scanned_gradient, gate_grad_in = pull_norm(normed_grad)
    input_grad, step_grad, b_grad, c_grad = pull_back(scanned_gradient)
    return (grad_gate, grad_up, grad_down, grad_out_proj, input_grad.reshape(TOKENS, DI).astype(jnp.bfloat16), step_grad, b_grad.reshape(TOKENS, GROUPS * STATE).astype(jnp.bfloat16), c_grad.reshape(TOKENS, GROUPS * STATE).astype(jnp.bfloat16), gate_grad_in.astype(jnp.bfloat16))
```

```python
import functools

import jax
import jax.numpy as jnp
from jax import lax
from jax.experimental import pallas as pl
from jax.experimental.pallas import tpu as pltpu
from jax.sharding import PartitionSpec as P

HDIM = 64
STATE = 128
BLK = 128


norm_eps = 1e-05
exact_mode = lax.Precision.HIGH


MESH = pl.DeviceIdType.MESH
BF16 = jnp.bfloat16
F32 = jnp.float32
DMA = pltpu.SemaphoreType.DMA


class Place:
    def __init__(self, n_sp, n_tp):
        self.n_sp, self.n_tp = n_sp, n_tp
        self.inner = 2 if n_tp % 2 == 0 else 1
        self.outer = n_tp // self.inner
        self.me = lax.axis_index("sp")
        self.t = lax.axis_index("tp")
        self.core = lax.rem(self.t, self.inner)
        self.far = lax.div(self.t, self.inner)

    def span(self, d):
        return lax.rem(self.me + d, self.n_sp)

    def span_back(self, d):
        return lax.rem(self.me + (self.n_sp - d), self.n_sp)

    def partners(self):
        return [self.far * self.inner + lax.rem(self.core + i, self.inner) for i in range(1, self.inner)]

    def outers(self):
        return [lax.rem(self.far + j, self.outer) * self.inner + self.core for j in range(1, self.outer)]

    def enter(self, with_span=True):
        barrier = pltpu.get_barrier_semaphore()
        devices = [(self.me, p) for p in self.partners() + self.outers()]
        if with_span:
            devices += [(self.span(d), self.t) for d in range(1, self.n_sp)]
        for device in devices:
            pl.semaphore_signal(barrier, inc=1, device_id=device, device_id_type=MESH)
        pl.semaphore_wait(barrier, len(devices))


def remote(src, dst, send, recv, device):
    return pltpu.make_async_remote_copy(
        src_ref=src, dst_ref=dst, send_sem=send, recv_sem=recv, device_id=device, device_id_type=MESH
    )


def decay_column(row, per):
    width = row.shape[-1]
    down = lax.broadcasted_iota(jnp.int32, (per, width), 0)
    across = lax.broadcasted_iota(jnp.int32, (per, width), 1)
    spread = jnp.broadcast_to(row.astype(F32), (per, width))
    return jnp.sum(jnp.where(down == across, spread, 0.0), axis=1, keepdims=True)


def dispatch_kernel(
    n_sp,
    n_tp,
    rows_ref,
    grads_ref,
    state_ref,
    first_ref,
    rows_out,
    grads_out,
    before_out,
    decays_out,
    state_in,
    before_tmp,
    span_send,
    tp_send,
    fwd_send,
    block_recv,
    state_send,
    state_recv,
    back_send,
    back_recv,
):
    at = Place(n_sp, n_tp)
    me, t = at.me, at.t
    width = rows_ref.shape[2]
    per = first_ref.shape[0]

    def cols(owner):
        return pl.ds(pl.multiple_of(owner * width, width), width)

    pairs = ((rows_ref, rows_out), (grads_ref, grads_out))
    at.enter()
    waits = []
    for d in range(1, n_sp):
        peer = at.span(d)
        for a, (src, dst) in enumerate(pairs):
            copy = remote(
                src.at[peer],
                dst.at[me, :, cols(t)],
                span_send.at[a, d],
                block_recv.at[a, me, t],
                (peer, t),
            )
            copy.start()
            waits.append(copy.wait_send)
    for d in range(1, n_sp):
        peer = at.span(d)
        copy = remote(
            state_ref.at[peer], state_in.at[me], state_send.at[d], state_recv.at[me], (peer, t)
        )
        copy.start()
        waits.append(copy.wait_send)

    def pass_on(d, sources, peers, owner, sems, base):
        src_span = at.span_back(d)
        for a in range(2):
            for i, peer in enumerate(peers):
                copy = remote(
                    sources[a],
                    pairs[a][1].at[src_span, :, cols(owner)],
                    sems.at[a, d, base + i],
                    block_recv.at[a, src_span, owner],
                    (me, peer),
                )
                copy.start()
                waits.append(copy.wait_send)

    def landed(a, src_span, owner):
        block = pairs[a][1].at[src_span, :, cols(owner)]
        pltpu.make_async_copy(block, block, block_recv.at[a, src_span, owner]).wait()

    near = at.outers() + at.partners()
    pass_on(0, [rows_ref.at[me], grads_ref.at[me]], near, t, tp_send, 0)
    rows_out[me, :, cols(t)] = rows_ref[me]
    grads_out[me, :, cols(t)] = grads_ref[me]
    state_in[me] = state_ref[me]
    for d in range(1, n_sp):
        src_span = at.span_back(d)
        for a in range(2):
            landed(a, src_span, t)
        pass_on(d, [p[1].at[src_span, :, cols(t)] for p in pairs], near, t, tp_send, 0)

    for d in range(1, n_sp):
        src_span = at.span_back(d)
        block = state_in.at[src_span]
        pltpu.make_async_copy(block, block, state_recv.at[src_span]).wait()
    running = first_ref[...]
    for k in range(n_sp):
        before_tmp[k] = running.astype(BF16)
        line = state_in[k, per : per + 1]
        decays_out[k] = line
        running = decay_column(line, per) * running + state_in[k, :per].astype(F32)
    for d in range(1, n_sp):
        peer = at.span(d)
        copy = remote(
            before_tmp.at[peer], before_out.at[me], back_send.at[d], back_recv.at[me], (peer, t)
        )
        copy.start()
        waits.append(copy.wait_send)
    before_out[me] = before_tmp[me]

    for d in range(n_sp):
        src_span = at.span_back(d)
        for j, owner in enumerate(at.outers()):
            for a in range(2):
                landed(a, src_span, owner)
            pass_on(
                d,
                [p[1].at[src_span, :, cols(owner)] for p in pairs],
                at.partners(),
                owner,
                fwd_send,
                j * (at.inner - 1),
            )
    for d in range(n_sp):
        src_span = at.span_back(d)
        for partner in at.partners():
            core = lax.rem(partner, at.inner)
            for far in range(at.outer):
                for a in range(2):
                    landed(a, src_span, far * at.inner + core)
    for d in range(1, n_sp):
        src_span = at.span_back(d)
        block = before_out.at[src_span]
        pltpu.make_async_copy(block, block, back_recv.at[src_span]).wait()
    for wait in waits:
        wait()


def whole(count):
    return [pl.BlockSpec(memory_space=pltpu.VMEM)] * count


def dispatch(rows, grads, state, first, n_tp):
    n_sp, capacity, width = rows.shape
    per, lanes = first.shape
    inner = 2 if n_tp % 2 == 0 else 1
    near = n_tp // inner - 1 + inner - 1
    out = jax.ShapeDtypeStruct((n_sp, capacity, width * n_tp), BF16)
    return pl.pallas_call(
        functools.partial(dispatch_kernel, n_sp, n_tp),
        out_shape=(
            out,
            out,
            jax.ShapeDtypeStruct((n_sp, per, lanes), BF16),
            jax.ShapeDtypeStruct((n_sp, 1, lanes), BF16),
        ),
        in_specs=whole(4),
        out_specs=tuple(whole(4)),
        scratch_shapes=[
            pltpu.VMEM(state.shape, BF16),
            pltpu.VMEM((n_sp, per, lanes), BF16),
            DMA((2, n_sp)),
            DMA((2, n_sp, max(near, 1))),
            DMA((2, n_sp, max((n_tp // inner - 1) * (inner - 1), 1))),
            DMA((2, n_sp, n_tp)),
            DMA((n_sp,)),
            DMA((n_sp,)),
            DMA((n_sp,)),
            DMA((n_sp,)),
        ],
        compiler_params=pltpu.CompilerParams(collective_id=1, has_side_effects=True),
        cost_estimate=pl.CostEstimate(
            flops=20_000_000_000, bytes_accessed=8_000_000, transcendentals=0
        ),
        name="dispatch",
    )(rows, grads, state, first)


def return_kernel(
    n_sp,
    n_tp,
    part_ref,
    grad_ref,
    pick_ref,
    mix_out,
    pair_in,
    far_out,
    far_in,
    ret_out,
    ret_in,
    own,
    pair_send,
    pair_recv,
    far_send,
    far_recv,
    ret_send,
    ret_recv,
    mix_send,
    mix_recv,
):
    at = Place(n_sp, n_tp)
    me, t = at.me, at.t
    width = grad_ref.shape[1]

    def cols(owner):
        return pl.ds(pl.multiple_of(owner * width, width), width)

    at.enter()
    waits = []
    order = list(range(1, n_sp)) + [0]
    for d in order:
        span = at.span(d)
        for i, partner in enumerate(at.partners()):
            core = lax.rem(partner, at.inner)
            for far in range(at.outer):
                copy = remote(
                    part_ref.at[span, :, cols(far * at.inner + core)],
                    pair_in.at[i, far, span],
                    pair_send.at[i, far, d],
                    pair_recv.at[i, far, span],
                    (me, partner),
                )
                copy.start()
                waits.append(copy.wait_send)

    def landed(block, sem):
        pltpu.make_async_copy(block, block, sem).wait()

    def pair_sum(span, far):
        total = part_ref[span, :, cols(far * at.inner + at.core)].astype(F32)
        for i in range(at.inner - 1):
            total = total + pair_in[i, far, span].astype(F32)
        return total

    for d in order:
        span = at.span(d)
        for i in range(at.inner - 1):
            for far in range(at.outer):
                landed(pair_in.at[i, far, span], pair_recv.at[i, far, span])
        for j in range(1, at.outer):
            far = lax.rem(at.far + j, at.outer)
            far_out[j - 1, span] = pair_sum(span, far).astype(BF16)
            copy = remote(
                far_out.at[j - 1, span],
                far_in.at[j - 1, span],
                far_send.at[j - 1, d],
                far_recv.at[j - 1, span],
                (me, far * at.inner + at.core),
            )
            copy.start()
            waits.append(copy.wait_send)
    for d in order:
        span = at.span(d)
        total = pair_sum(span, at.far)
        for j in range(1, at.outer):
            landed(far_in.at[j - 1, span], far_recv.at[j - 1, span])
            total = total + far_in[j - 1, span].astype(F32)
        if d == 0:
            ret_in[me] = total.astype(BF16)
        else:
            ret_out[span] = total.astype(BF16)
            copy = remote(
                ret_out.at[span], ret_in.at[me], ret_send.at[d], ret_recv.at[me], (span, t)
            )
            copy.start()
            waits.append(copy.wait_send)
    total = grad_ref[...].astype(F32)
    total = total + jnp.dot(pick_ref[me], ret_in[me], preferred_element_type=F32)
    for d in range(1, n_sp):
        span = at.span_back(d)
        landed(ret_in.at[span], ret_recv.at[span])
        total = total + jnp.dot(pick_ref[span], ret_in[span], preferred_element_type=F32)
    own[...] = total.astype(BF16)
    mix_out[:, cols(t)] = total.astype(BF16)
    near = at.outers() + at.partners()
    for i, peer in enumerate(near):
        copy = remote(own, mix_out.at[:, cols(t)], mix_send.at[0, i], mix_recv.at[t], (me, peer))
        copy.start()
        waits.append(copy.wait_send)
    for j, owner in enumerate(at.outers()):
        block = mix_out.at[:, cols(owner)]
        landed(block, mix_recv.at[owner])
        for i, partner in enumerate(at.partners()):
            copy = remote(
                block, block, mix_send.at[1 + j, i], mix_recv.at[owner], (me, partner)
            )
            copy.start()
            waits.append(copy.wait_send)
    for partner in at.partners():
        core = lax.rem(partner, at.inner)
        for far in range(at.outer):
            owner = far * at.inner + core
            landed(mix_out.at[:, cols(owner)], mix_recv.at[owner])
    for wait in waits:
        wait()


def return_rows(partial, grad_rows, pick, n_tp):
    n_sp, capacity, model_width = partial.shape
    tokens, width = grad_rows.shape
    inner = 2 if n_tp % 2 == 0 else 1
    outer = n_tp // inner
    blocks = (n_sp, capacity, width)
    return pl.pallas_call(
        functools.partial(return_kernel, n_sp, n_tp),
        out_shape=jax.ShapeDtypeStruct((tokens, model_width), BF16),
        in_specs=whole(3),
        out_specs=whole(1)[0],
        scratch_shapes=[
            pltpu.VMEM((max(inner - 1, 1), outer) + blocks, BF16),
            pltpu.VMEM((max(outer - 1, 1),) + blocks, BF16),
            pltpu.VMEM((max(outer - 1, 1),) + blocks, BF16),
            pltpu.VMEM(blocks, BF16),
            pltpu.VMEM(blocks, BF16),
            pltpu.VMEM((tokens, width), BF16),
            DMA((max(inner - 1, 1), outer, n_sp)),
            DMA((max(inner - 1, 1), outer, n_sp)),
            DMA((max(outer - 1, 1), n_sp)),
            DMA((max(outer - 1, 1), n_sp)),
            DMA((n_sp,)),
            DMA((n_sp,)),
            DMA((outer, n_tp)),
            DMA((n_tp,)),
        ],
        compiler_params=pltpu.CompilerParams(collective_id=2, has_side_effects=True),
        cost_estimate=pl.CostEstimate(
            flops=20_000_000_000, bytes_accessed=8_000_000, transcendentals=0
        ),
        name="return_rows",
    )(partial, grad_rows, pick)


def after_kernel(
    n_sp,
    n_tp,
    reached_ref,
    decays_ref,
    mix_ref,
    later_out,
    mix_out,
    reached_in,
    after_tmp,
    reach_send,
    reach_recv,
    back_send,
    back_recv,
    mix_send,
    mix_recv,
    fwd_send,
    fwd_recv,
):
    at = Place(n_sp, n_tp)
    me, t = at.me, at.t
    per = reached_ref.shape[1]
    half = mix_ref.shape[1] // at.inner

    def share(core):
        return pl.ds(pl.multiple_of(core * half, half), half)

    def landed(block, sem):
        pltpu.make_async_copy(block, block, sem).wait()

    at.enter()
    waits = []
    for d in range(1, n_sp):
        peer = at.span(d)
        copy = remote(
            reached_ref.at[peer], reached_in.at[me], reach_send.at[d], reach_recv.at[me], (peer, t)
        )
        copy.start()
        waits.append(copy.wait_send)
    for d in range(1, n_sp):
        peer = at.span(d)
        copy = remote(
            mix_ref.at[peer, share(at.core)],
            mix_out.at[me, share(at.core)],
            mix_send.at[d],
            mix_recv.at[me],
            (peer, t),
        )
        copy.start()
        waits.append(copy.wait_send)
    reached_in[me] = reached_ref[me]
    mix_out[me] = mix_ref[me]
    for d in range(1, n_sp):
        src_span = at.span_back(d)
        landed(reached_in.at[src_span], reach_recv.at[src_span])
    running = jnp.zeros(reached_ref.shape[1:], F32)
    for k in reversed(range(n_sp)):
        after_tmp[k] = running.astype(BF16)
        running = decay_column(decays_ref[k], per) * running + reached_in[k].astype(F32)
    for d in range(1, n_sp):
        peer = at.span(d)
        copy = remote(
            after_tmp.at[peer], later_out.at[me], back_send.at[d], back_recv.at[me], (peer, t)
        )
        copy.start()
        waits.append(copy.wait_send)
    later_out[me] = after_tmp[me]
    for d in range(1, n_sp):
        src_span = at.span_back(d)
        block = mix_out.at[src_span, share(at.core)]
        landed(block, mix_recv.at[src_span])
        for i, partner in enumerate(at.partners()):
            copy = remote(
                block, block, fwd_send.at[i, d], fwd_recv.at[i, src_span], (me, partner)
            )
            copy.start()
            waits.append(copy.wait_send)
    for d in range(1, n_sp):
        src_span = at.span_back(d)
        for i, partner in enumerate(at.partners()):
            landed(
                mix_out.at[src_span, share(lax.rem(partner, at.inner))], fwd_recv.at[i, src_span]
            )
        landed(later_out.at[src_span], back_recv.at[src_span])
    for wait in waits:
        wait()


def gradient_after(reached, decays, mix, n_tp):
    n_sp = reached.shape[0]
    inner = 2 if n_tp % 2 == 0 else 1
    return pl.pallas_call(
        functools.partial(after_kernel, n_sp, n_tp),
        out_shape=(
            jax.ShapeDtypeStruct(reached.shape, BF16),
            jax.ShapeDtypeStruct(mix.shape, BF16),
        ),
        in_specs=whole(3),
        out_specs=tuple(whole(2)),
        scratch_shapes=[
            pltpu.VMEM(reached.shape, BF16),
            pltpu.VMEM(reached.shape, BF16),
            DMA((n_sp,)),
            DMA((n_sp,)),
            DMA((n_sp,)),
            DMA((n_sp,)),
            DMA((n_sp,)),
            DMA((n_sp,)),
            DMA((max(inner - 1, 1), n_sp)),
            DMA((max(inner - 1, 1), n_sp)),
        ],
        compiler_params=pltpu.CompilerParams(collective_id=3, has_side_effects=True),
        cost_estimate=pl.CostEstimate(
            flops=15_000_000_000, bytes_accessed=4_000_000, transcendentals=0
        ),
        name="gradient_after",
    )(reached, decays, mix)


def pack_state(state, decay, count):
    width = state.shape[-1]
    per = state.shape[0] * state.shape[1] // count
    row_decay = jnp.repeat(decay, state.shape[1]).reshape(count, per)
    lines = -(-per // width)
    row_decay = jnp.pad(row_decay, ((0, 0), (0, lines * width - per)))
    return jnp.concatenate(
        [state.reshape(count, per, width), row_decay.reshape(count, lines, width)], axis=1
    ).astype(BF16)


def span_local_scan(
    input_heads,
    time_step,
    decay_speed,
    sudden_decay,
    input_vector_groups,
    readout_groups,
    starting_state,
):
    length, head_count, head_size = input_heads.shape
    groups, state_size = (input_vector_groups.shape[1], input_vector_groups.shape[2])
    per_group = head_count // groups
    block_count = length // BLK
    log_decay_total = sudden_decay - time_step * decay_speed[None, :]
    scaled = (input_heads * time_step[:, :, None]).reshape(
        block_count, BLK, groups, per_group, head_size
    )
    log_decay_total = log_decay_total.reshape(block_count, BLK, groups, per_group)
    b_rows = input_vector_groups.reshape(block_count, BLK, groups, state_size)
    c_rows = readout_groups.reshape(block_count, BLK, groups, state_size)
    cumulative = jnp.cumsum(log_decay_total, axis=1)
    causal_mask = jnp.tril(jnp.ones((BLK, BLK), dtype=bool))
    cum_t = jnp.moveaxis(cumulative, 1, -1)
    gaps = cum_t[..., :, None] - cum_t[..., None, :]
    decays = jnp.where(causal_mask, jnp.exp(jnp.where(causal_mask, gaps, 0.0)), 0.0)
    affinity = jnp.einsum("blgn,bsgn->bgls", c_rows, b_rows, precision=exact_mode)
    y_diag = jnp.einsum(
        "bghls,bsghp->blghp", affinity[:, :, None] * decays, scaled, precision=exact_mode
    )
    to_end = jnp.exp(cumulative[:, -1:] - cumulative)
    states = jnp.einsum(
        "blgn,blghp->bghpn", b_rows, scaled * to_end[..., None], precision=exact_mode
    )
    block_decay = jnp.exp(cumulative[:, -1])

    def advance(running, inputs):
        block_state, decay_now = inputs
        return (decay_now[..., None, None] * running + block_state, running)

    first_state = starting_state.reshape(groups, per_group, head_size, state_size)
    closing_state, incoming_state = lax.scan(advance, first_state, (states, block_decay))
    y_off = (
        jnp.einsum("blgn,bghpn->blghp", c_rows, incoming_state, precision=exact_mode)
        * jnp.exp(cumulative)[..., None]
    )
    result_rows = (y_diag + y_off).reshape(length, head_count, head_size)
    return (result_rows, closing_state.reshape(head_count, head_size, state_size))


def span_final_state(input_heads, time_step, decay_speed, sudden_decay, input_vector_groups):
    length, head_count, head_size = input_heads.shape
    groups = input_vector_groups.shape[1]
    log_decay_total = sudden_decay - time_step * decay_speed[None, :]
    sum_total = jnp.sum(log_decay_total, axis=0)
    after = sum_total[None, :] - jnp.cumsum(log_decay_total, axis=0)
    weighted = (input_heads * (time_step * jnp.exp(after))[:, :, None]).reshape(
        length, groups, head_count // groups, head_size
    )
    result = jnp.einsum("tgn,tghp->ghpn", input_vector_groups, weighted, precision=exact_mode)
    return (result.reshape(head_count, head_size, -1), jnp.exp(sum_total))


def carried_weight(scanned_gradient, readout_groups, time_step, decay_speed, sudden_decay):
    length, head_count, head_size = scanned_gradient.shape
    groups = readout_groups.shape[1]
    log_decay_total = sudden_decay - time_step * decay_speed[None, :]
    weighted = (
        scanned_gradient * jnp.exp(jnp.cumsum(log_decay_total, axis=0))[:, :, None]
    ).reshape(length, groups, head_count // groups, head_size)
    result = jnp.einsum("tgn,tghp->ghpn", readout_groups, weighted, precision=exact_mode)
    return result.reshape(head_count, head_size, -1)


def gate_norm(scan_out, gate_vals, group_norm_scale, groups):
    length = scan_out.shape[0]
    gated = scan_out.reshape(length, -1) * jax.nn.silu(gate_vals)
    grouped = gated.reshape(length, groups, -1)
    factor = lax.rsqrt(jnp.mean(grouped * grouped, axis=-1, keepdims=True) + norm_eps)
    return (grouped * factor).reshape(length, -1) * group_norm_scale[None, :]


def slot_choice(route_rows, expert_count, capacity):
    flat_routes = route_rows.reshape(-1)
    pairs = flat_routes.shape[0]
    onehot = flat_routes[:, None] == jnp.arange(expert_count, dtype=jnp.int32)[None, :]
    earlier = jnp.tril(jnp.ones((pairs, pairs), jnp.bfloat16), -1)
    before = jnp.dot(earlier, onehot.astype(jnp.bfloat16), preferred_element_type=jnp.float32)
    place = jnp.sum(jnp.where(onehot, before, 0.0), axis=1).astype(jnp.int32)
    destination = (flat_routes * capacity + place).reshape(route_rows.shape)
    slots = jnp.arange(expert_count * capacity, dtype=jnp.int32)
    return [slots[:, None] == destination[None, :, k] for k in range(route_rows.shape[1])]


def pack_rows(stream, grad_rows, chosen, weights):
    pick = sum(c.astype(jnp.bfloat16) for c in chosen)
    weight_of = sum(
        jnp.sum(jnp.where(c, weights[None, :, k], 0.0), axis=1) for k, c in enumerate(chosen)
    )
    routed = jnp.dot(pick, stream, preferred_element_type=jnp.float32).astype(jnp.bfloat16)
    picked = jnp.dot(pick, grad_rows, preferred_element_type=jnp.float32)
    return (routed, (picked * weight_of[:, None]).astype(jnp.bfloat16), pick)


def expert_hidden(routed_rows, routed_grads, w_gate, w_up, w_down):
    pre_gate = jnp.dot(routed_rows, w_gate, preferred_element_type=jnp.float32)
    pre_up = jnp.dot(routed_rows, w_up, preferred_element_type=jnp.float32)
    activated = jax.nn.silu(pre_gate)
    hidden = (activated * pre_up).astype(jnp.bfloat16)
    hidden_grad = lax.dot_general(
        routed_grads, w_down, (((1,), (1,)), ((), ())), preferred_element_type=jnp.float32
    )
    sigmoid_gate = jax.nn.sigmoid(pre_gate)
    gate_grad = (
        hidden_grad * pre_up * sigmoid_gate * (1.0 + pre_gate * (1.0 - sigmoid_gate))
    ).astype(jnp.bfloat16)
    up_grad = (hidden_grad * activated).astype(jnp.bfloat16)
    return (hidden, gate_grad, up_grad)


def expert_weight_grads(routed_rows, routed_grads, hidden, gate_grad, up_grad):
    contract = (((0,), (0,)), ((), ()))
    grad_g = lax.dot_general(routed_rows, gate_grad, contract, preferred_element_type=jnp.float32)
    grad_u = lax.dot_general(routed_rows, up_grad, contract, preferred_element_type=jnp.float32)
    grad_d = lax.dot_general(hidden, routed_grads, contract, preferred_element_type=jnp.float32)
    return (grad_g.astype(jnp.bfloat16), grad_u.astype(jnp.bfloat16), grad_d.astype(jnp.bfloat16))


def row_partial(gate_grad, up_grad, w_gate, w_up):
    contract = (((1,), (1,)), ((), ()))
    partial_sum = lax.dot_general(gate_grad, w_gate, contract, preferred_element_type=jnp.float32)
    partial_sum = partial_sum + lax.dot_general(
        up_grad, w_up, contract, preferred_element_type=jnp.float32
    )
    return lax.optimization_barrier(partial_sum.astype(jnp.bfloat16)).astype(jnp.float32)


def body(
    mixer_output_stream,
    layer_output_gradient,
    routes,
    expert_combine_weight,
    expert_gate_weight,
    expert_up_weight,
    expert_down_weight,
    head_mixer_input,
    head_step_size,
    head_decay_rate,
    extra_log_decay,
    state_entering_span,
    state_input_vectors,
    state_readout_vectors,
    gate_preactivation,
    group_norm_scale,
    mixer_output_weight,
):
    expert_count = lax.axis_size("sp")
    local_tokens = routes.shape[0]
    capacity = 3 * local_tokens // expert_count
    chosen = slot_choice(routes, expert_count, capacity)
    w_gate = expert_gate_weight[0]
    w_up = expert_up_weight[0]
    w_down = expert_down_weight[0]
    sent_rows, sent_grads, pick = pack_rows(
        mixer_output_stream, layer_output_gradient, chosen, expert_combine_weight
    )
    whole_weight = lax.all_gather(mixer_output_weight, "sp", axis=1, tiled=True)
    n_tp = lax.axis_size("tp")
    head_local = head_step_size.shape[1]
    group_local = state_input_vectors.shape[1] // STATE
    input_heads = head_mixer_input.astype(jnp.float32).reshape(local_tokens, head_local, HDIM)
    input_vector_groups = state_input_vectors.astype(jnp.float32).reshape(
        local_tokens, group_local, STATE
    )
    readout_groups = state_readout_vectors.astype(jnp.float32).reshape(
        local_tokens, group_local, STATE
    )
    within_span_state, within_span_decay = span_final_state(
        input_heads, head_step_size, head_decay_rate, extra_log_decay, input_vector_groups
    )
    state_shape = within_span_state.shape
    state_rows = state_shape[0] * state_shape[1]
    per_span = state_rows // expert_count
    first_rows = lax.dynamic_slice_in_dim(
        state_entering_span.reshape(state_rows, STATE), lax.axis_index("sp") * per_span, per_span, 0
    )
    routed_rows, routed_grads, before, span_decays = dispatch(
        sent_rows.reshape(expert_count, capacity, -1),
        sent_grads.reshape(expert_count, capacity, -1),
        pack_state(within_span_state, within_span_decay, expert_count),
        first_rows,
        n_tp,
    )
    incoming_state = before.astype(jnp.float32).reshape(state_shape)

    def forward(input_values, time_step_values, input_vector_entries, readout_entries):
        return span_local_scan(
            input_values,
            time_step_values,
            head_decay_rate,
            extra_log_decay,
            input_vector_entries,
            readout_entries,
            incoming_state,
        )

    (scan_out, closing_state), pull_back = jax.vjp(
        forward, input_heads, head_step_size, input_vector_groups, readout_groups
    )

    def apply_norm(scan_vals, gate_vals):
        return gate_norm(scan_vals, gate_vals, group_norm_scale, group_local)

    normed, pull_norm = jax.vjp(apply_norm, scan_out, gate_preactivation.astype(jnp.float32))
    normed_low = normed.astype(jnp.bfloat16)
    normed_all = lax.all_gather(normed_low, "sp", axis=0, tiled=True)
    routed_rows, normed_low = lax.optimization_barrier((routed_rows, normed_low))
    model_width = routed_rows.shape[2]
    routed_rows = routed_rows.reshape(-1, model_width)
    routed_grads = routed_grads.reshape(-1, model_width)
    hidden, gate_grad, up_grad = expert_hidden(routed_rows, routed_grads, w_gate, w_up, w_down)
    grad_g, grad_u, grad_d = expert_weight_grads(
        routed_rows, routed_grads, hidden, gate_grad, up_grad
    )
    partial_rows = row_partial(gate_grad, up_grad, w_gate, w_up)
    partial_rows = partial_rows.astype(jnp.bfloat16).reshape(expert_count, capacity, model_width)
    mix_grad = return_rows(
        partial_rows,
        layer_output_gradient,
        pick.reshape(expert_count, capacity, local_tokens).swapaxes(1, 2),
        n_tp,
    )
    columns = mix_grad
    normed_grad = lax.dot_general(
        columns,
        whole_weight,
        (((1,), (1,)), ((), ())),
        preferred_element_type=jnp.float32,
    )
    scanned_gradient, gate_grad_in = pull_norm(normed_grad)
    reached_gradient = carried_weight(
        scanned_gradient, readout_groups, head_step_size, head_decay_rate, extra_log_decay
    )
    later_grad, mix_columns = gradient_after(
        reached_gradient.astype(jnp.bfloat16).reshape(before.shape),
        span_decays,
        mix_grad.reshape(local_tokens, expert_count, -1).swapaxes(0, 1),
        n_tp,
    )
    later_grad = later_grad.astype(jnp.float32).reshape(state_shape)
    mix_columns = mix_columns.reshape(expert_count * local_tokens, -1)
    proj_grad = lax.dot_general(
        normed_all, mix_columns, (((0,), (0,)), ((), ())), preferred_element_type=jnp.float32
    )
    input_grad, step_grad, b_grad, c_grad = pull_back((scanned_gradient, later_grad))
    return (
        grad_g[None],
        grad_u[None],
        grad_d[None],
        proj_grad,
        input_grad.reshape(local_tokens, -1).astype(jnp.bfloat16),
        step_grad,
        b_grad.reshape(local_tokens, -1).astype(jnp.bfloat16),
        c_grad.reshape(local_tokens, -1).astype(jnp.bfloat16),
        gate_grad_in.astype(jnp.bfloat16),
    )


def solution(mesh):
    return jax.shard_map(
        body,
        mesh=mesh,
        in_specs=(
            P("sp", "tp"),
            P("sp", "tp"),
            P("sp", None),
            P("sp", None),
            P("sp", None, "tp"),
            P("sp", None, "tp"),
            P("sp", "tp", None),
            P("sp", "tp"),
            P("sp", "tp"),
            P("tp"),
            P("sp", "tp"),
            P("tp", None, None),
            P("sp", "tp"),
            P("sp", "tp"),
            P("sp", "tp"),
            P("tp"),
            P("tp", "sp"),
        ),
        out_specs=(
            P("sp", None, "tp"),
            P("sp", None, "tp"),
            P("sp", "tp", None),
            P("tp", "sp"),
            P("sp", "tp"),
            P("sp", "tp"),
            P("sp", "tp"),
            P("sp", "tp"),
            P("sp", "tp"),
        ),
        check_vma=False,
    )
```

```python
import functools

import jax
import jax.numpy as jnp
from jax import lax
from jax.experimental import pallas as pl
from jax.experimental.pallas import tpu as pltpu
from jax.sharding import PartitionSpec as P

HDIM = 64
STATE = 128
BLK = 128


norm_eps = 1e-05
exact_mode = lax.Precision.HIGH


MESH = pl.DeviceIdType.MESH
BF16 = jnp.bfloat16
F32 = jnp.float32
DMA = pltpu.SemaphoreType.DMA


class Place:
    def __init__(self, n_sp, n_tp):
        self.n_sp, self.n_tp = n_sp, n_tp
        self.inner = 2 if n_tp % 2 == 0 else 1
        self.outer = n_tp // self.inner
        self.me = lax.axis_index("sp")
        self.t = lax.axis_index("tp")
        self.core = lax.rem(self.t, self.inner)
        self.far = lax.div(self.t, self.inner)

    def span(self, d):
        return lax.rem(self.me + d, self.n_sp)

    def span_back(self, d):
        return lax.rem(self.me + (self.n_sp - d), self.n_sp)

    def partners(self):
        return [self.far * self.inner + lax.rem(self.core + i, self.inner) for i in range(1, self.inner)]

    def outers(self):
        return [lax.rem(self.far + j, self.outer) * self.inner + self.core for j in range(1, self.outer)]

    def enter(self, with_span=True):
        barrier = pltpu.get_barrier_semaphore()
        devices = [(self.me, p) for p in self.partners() + self.outers()]
        if with_span:
            devices += [(self.span(d), self.t) for d in range(1, self.n_sp)]
        for device in devices:
            pl.semaphore_signal(barrier, inc=1, device_id=device, device_id_type=MESH)
        pl.semaphore_wait(barrier, len(devices))


def remote(src, dst, send, recv, device):
    return pltpu.make_async_remote_copy(
        src_ref=src, dst_ref=dst, send_sem=send, recv_sem=recv, device_id=device, device_id_type=MESH
    )


def decay_column(row, per):
    width = row.shape[-1]
    down = lax.broadcasted_iota(jnp.int32, (per, width), 0)
    across = lax.broadcasted_iota(jnp.int32, (per, width), 1)
    spread = jnp.broadcast_to(row.astype(F32), (per, width))
    return jnp.sum(jnp.where(down == across, spread, 0.0), axis=1, keepdims=True)


def dispatch_kernel(
    n_sp,
    n_tp,
    rows_ref,
    grads_ref,
    state_ref,
    rows_out,
    grads_out,
    state_in,
    span_send,
    tp_send,
    fwd_send,
    block_recv,
    state_send,
    state_recv,
):
    at = Place(n_sp, n_tp)
    me, t = at.me, at.t
    width = rows_ref.shape[2]

    def cols(owner):
        return pl.ds(pl.multiple_of(owner * width, width), width)

    pairs = ((rows_ref, rows_out), (grads_ref, grads_out))
    at.enter()
    waits = []
    for d in range(1, n_sp):
        peer = at.span(d)
        for a, (src, dst) in enumerate(pairs):
            copy = remote(
                src.at[peer],
                dst.at[me, :, cols(t)],
                span_send.at[a, d],
                block_recv.at[a, me, t],
                (peer, t),
            )
            copy.start()
            waits.append(copy.wait_send)
    for d in range(1, n_sp):
        peer = at.span(d)
        copy = remote(
            state_ref.at[peer], state_in.at[me], state_send.at[d], state_recv.at[me], (peer, t)
        )
        copy.start()
        waits.append(copy.wait_send)

    def pass_on(d, sources, peers, owner, sems, base):
        src_span = at.span_back(d)
        for a in range(2):
            for i, peer in enumerate(peers):
                copy = remote(
                    sources[a],
                    pairs[a][1].at[src_span, :, cols(owner)],
                    sems.at[a, d, base + i],
                    block_recv.at[a, src_span, owner],
                    (me, peer),
                )
                copy.start()
                waits.append(copy.wait_send)

    def landed(a, src_span, owner):
        block = pairs[a][1].at[src_span, :, cols(owner)]
        pltpu.make_async_copy(block, block, block_recv.at[a, src_span, owner]).wait()

    near = at.outers() + at.partners()
    pass_on(0, [rows_ref.at[me], grads_ref.at[me]], near, t, tp_send, 0)
    rows_out[me, :, cols(t)] = rows_ref[me]
    grads_out[me, :, cols(t)] = grads_ref[me]
    state_in[me] = state_ref[me]
    for d in range(1, n_sp):
        src_span = at.span_back(d)
        for a in range(2):
            landed(a, src_span, t)
        pass_on(d, [p[1].at[src_span, :, cols(t)] for p in pairs], near, t, tp_send, 0)

    for d in range(n_sp):
        src_span = at.span_back(d)
        for j, owner in enumerate(at.outers()):
            for a in range(2):
                landed(a, src_span, owner)
            pass_on(
                d,
                [p[1].at[src_span, :, cols(owner)] for p in pairs],
                at.partners(),
                owner,
                fwd_send,
                j * (at.inner - 1),
            )
    for d in range(n_sp):
        src_span = at.span_back(d)
        for partner in at.partners():
            core = lax.rem(partner, at.inner)
            for far in range(at.outer):
                for a in range(2):
                    landed(a, src_span, far * at.inner + core)
    for d in range(1, n_sp):
        src_span = at.span_back(d)
        block = state_in.at[src_span]
        pltpu.make_async_copy(block, block, state_recv.at[src_span]).wait()
    for wait in waits:
        wait()


def whole(count):
    return [pl.BlockSpec(memory_space=pltpu.VMEM)] * count


def dispatch(rows, grads, state, n_tp):
    n_sp, capacity, width = rows.shape
    inner = 2 if n_tp % 2 == 0 else 1
    near = n_tp // inner - 1 + inner - 1
    out = jax.ShapeDtypeStruct((n_sp, capacity, width * n_tp), BF16)
    return pl.pallas_call(
        functools.partial(dispatch_kernel, n_sp, n_tp),
        out_shape=(out, out, jax.ShapeDtypeStruct(state.shape, BF16)),
        in_specs=whole(3),
        out_specs=tuple(whole(3)),
        scratch_shapes=[
            DMA((2, n_sp)),
            DMA((2, n_sp, max(near, 1))),
            DMA((2, n_sp, max((n_tp // inner - 1) * (inner - 1), 1))),
            DMA((2, n_sp, n_tp)),
            DMA((n_sp,)),
            DMA((n_sp,)),
        ],
        compiler_params=pltpu.CompilerParams(collective_id=1, has_side_effects=True),
        cost_estimate=pl.CostEstimate(
            flops=20_000_000_000, bytes_accessed=8_000_000, transcendentals=0
        ),
        name="dispatch",
    )(rows, grads, state)


def return_kernel(
    n_sp,
    n_tp,
    part_ref,
    grad_ref,
    pick_ref,
    state_ref,
    first_ref,
    mix_out,
    before_out,
    decays_out,
    before_tmp,
    pair_in,
    far_out,
    far_in,
    ret_out,
    ret_in,
    own,
    pair_send,
    pair_recv,
    far_send,
    far_recv,
    ret_send,
    ret_recv,
    mix_send,
    mix_recv,
    back_send,
    back_recv,
):
    at = Place(n_sp, n_tp)
    me, t = at.me, at.t
    width = grad_ref.shape[1]
    per = first_ref.shape[0]

    def cols(owner):
        return pl.ds(pl.multiple_of(owner * width, width), width)

    at.enter()
    waits = []
    order = list(range(1, n_sp)) + [0]
    for d in order:
        span = at.span(d)
        for i, partner in enumerate(at.partners()):
            core = lax.rem(partner, at.inner)
            for far in range(at.outer):
                copy = remote(
                    part_ref.at[span, :, cols(far * at.inner + core)],
                    pair_in.at[i, far, span],
                    pair_send.at[i, far, d],
                    pair_recv.at[i, far, span],
                    (me, partner),
                )
                copy.start()
                waits.append(copy.wait_send)

    def landed(block, sem):
        pltpu.make_async_copy(block, block, sem).wait()

    def pair_sum(span, far):
        total = part_ref[span, :, cols(far * at.inner + at.core)].astype(F32)
        for i in range(at.inner - 1):
            total = total + pair_in[i, far, span].astype(F32)
        return total

    for d in order:
        span = at.span(d)
        for i in range(at.inner - 1):
            for far in range(at.outer):
                landed(pair_in.at[i, far, span], pair_recv.at[i, far, span])
        for j in range(1, at.outer):
            far = lax.rem(at.far + j, at.outer)
            far_out[j - 1, span] = pair_sum(span, far).astype(BF16)
            copy = remote(
                far_out.at[j - 1, span],
                far_in.at[j - 1, span],
                far_send.at[j - 1, d],
                far_recv.at[j - 1, span],
                (me, far * at.inner + at.core),
            )
            copy.start()
            waits.append(copy.wait_send)
    running = first_ref[...]
    for k in range(n_sp):
        before_tmp[k] = running.astype(BF16)
        line = state_ref[k, per : per + 1]
        decays_out[k] = line
        running = decay_column(line, per) * running + state_ref[k, :per].astype(F32)
    for d in range(1, n_sp):
        peer = at.span(d)
        copy = remote(
            before_tmp.at[peer], before_out.at[me], back_send.at[d], back_recv.at[me], (peer, t)
        )
        copy.start()
        waits.append(copy.wait_send)
    before_out[me] = before_tmp[me]
    for d in order:
        span = at.span(d)
        total = pair_sum(span, at.far)
        for j in range(1, at.outer):
            landed(far_in.at[j - 1, span], far_recv.at[j - 1, span])
            total = total + far_in[j - 1, span].astype(F32)
        if d == 0:
            ret_in[me] = total.astype(BF16)
        else:
            ret_out[span] = total.astype(BF16)
            copy = remote(
                ret_out.at[span], ret_in.at[me], ret_send.at[d], ret_recv.at[me], (span, t)
            )
            copy.start()
            waits.append(copy.wait_send)
    total = grad_ref[...].astype(F32)
    total = total + jnp.dot(pick_ref[me], ret_in[me], preferred_element_type=F32)
    for d in range(1, n_sp):
        span = at.span_back(d)
        landed(ret_in.at[span], ret_recv.at[span])
        total = total + jnp.dot(pick_ref[span], ret_in[span], preferred_element_type=F32)
    own[...] = total.astype(BF16)
    mix_out[:, cols(t)] = total.astype(BF16)
    near = at.outers() + at.partners()
    for i, peer in enumerate(near):
        copy = remote(own, mix_out.at[:, cols(t)], mix_send.at[0, i], mix_recv.at[t], (me, peer))
        copy.start()
        waits.append(copy.wait_send)
    for j, owner in enumerate(at.outers()):
        block = mix_out.at[:, cols(owner)]
        landed(block, mix_recv.at[owner])
        for i, partner in enumerate(at.partners()):
            copy = remote(
                block, block, mix_send.at[1 + j, i], mix_recv.at[owner], (me, partner)
            )
            copy.start()
            waits.append(copy.wait_send)
    for partner in at.partners():
        core = lax.rem(partner, at.inner)
        for far in range(at.outer):
            owner = far * at.inner + core
            landed(mix_out.at[:, cols(owner)], mix_recv.at[owner])
    for d in range(1, n_sp):
        src_span = at.span_back(d)
        landed(before_out.at[src_span], back_recv.at[src_span])
    for wait in waits:
        wait()


def return_rows(partial, grad_rows, pick, state, first, n_tp):
    n_sp, capacity, model_width = partial.shape
    tokens, width = grad_rows.shape
    per, lanes = first.shape
    inner = 2 if n_tp % 2 == 0 else 1
    outer = n_tp // inner
    blocks = (n_sp, capacity, width)
    return pl.pallas_call(
        functools.partial(return_kernel, n_sp, n_tp),
        out_shape=(
            jax.ShapeDtypeStruct((tokens, model_width), BF16),
            jax.ShapeDtypeStruct((n_sp, per, lanes), BF16),
            jax.ShapeDtypeStruct((n_sp, 1, lanes), BF16),
        ),
        in_specs=whole(5),
        out_specs=tuple(whole(3)),
        scratch_shapes=[
            pltpu.VMEM((n_sp, per, lanes), BF16),
            pltpu.VMEM((max(inner - 1, 1), outer) + blocks, BF16),
            pltpu.VMEM((max(outer - 1, 1),) + blocks, BF16),
            pltpu.VMEM((max(outer - 1, 1),) + blocks, BF16),
            pltpu.VMEM(blocks, BF16),
            pltpu.VMEM(blocks, BF16),
            pltpu.VMEM((tokens, width), BF16),
            DMA((max(inner - 1, 1), outer, n_sp)),
            DMA((max(inner - 1, 1), outer, n_sp)),
            DMA((max(outer - 1, 1), n_sp)),
            DMA((max(outer - 1, 1), n_sp)),
            DMA((n_sp,)),
            DMA((n_sp,)),
            DMA((outer, n_tp)),
            DMA((n_tp,)),
            DMA((n_sp,)),
            DMA((n_sp,)),
        ],
        compiler_params=pltpu.CompilerParams(collective_id=2, has_side_effects=True),
        cost_estimate=pl.CostEstimate(
            flops=20_000_000_000, bytes_accessed=8_000_000, transcendentals=0
        ),
        name="return_rows",
    )(partial, grad_rows, pick, state, first)


def after_kernel(
    n_sp,
    n_tp,
    reached_ref,
    decays_ref,
    mix_ref,
    later_out,
    mix_out,
    reached_in,
    after_tmp,
    reach_send,
    reach_recv,
    back_send,
    back_recv,
    mix_send,
    mix_recv,
    fwd_send,
    fwd_recv,
):
    at = Place(n_sp, n_tp)
    me, t = at.me, at.t
    per = reached_ref.shape[1]
    half = mix_ref.shape[1] // at.inner

    def share(core):
        return pl.ds(pl.multiple_of(core * half, half), half)

    def landed(block, sem):
        pltpu.make_async_copy(block, block, sem).wait()

    at.enter()
    waits = []
    for d in range(1, n_sp):
        peer = at.span(d)
        copy = remote(
            reached_ref.at[peer], reached_in.at[me], reach_send.at[d], reach_recv.at[me], (peer, t)
        )
        copy.start()
        waits.append(copy.wait_send)
    for d in range(1, n_sp):
        peer = at.span(d)
        copy = remote(
            mix_ref.at[peer, share(at.core)],
            mix_out.at[me, share(at.core)],
            mix_send.at[d],
            mix_recv.at[me],
            (peer, t),
        )
        copy.start()
        waits.append(copy.wait_send)
    reached_in[me] = reached_ref[me]
    mix_out[me] = mix_ref[me]
    for d in range(1, n_sp):
        src_span = at.span_back(d)
        landed(reached_in.at[src_span], reach_recv.at[src_span])
    running = jnp.zeros(reached_ref.shape[1:], F32)
    for k in reversed(range(n_sp)):
        after_tmp[k] = running.astype(BF16)
        running = decay_column(decays_ref[k], per) * running + reached_in[k].astype(F32)
    for d in range(1, n_sp):
        peer = at.span(d)
        copy = remote(
            after_tmp.at[peer], later_out.at[me], back_send.at[d], back_recv.at[me], (peer, t)
        )
        copy.start()
        waits.append(copy.wait_send)
    later_out[me] = after_tmp[me]
    for d in range(1, n_sp):
        src_span = at.span_back(d)
        block = mix_out.at[src_span, share(at.core)]
        landed(block, mix_recv.at[src_span])
        for i, partner in enumerate(at.partners()):
            copy = remote(
                block, block, fwd_send.at[i, d], fwd_recv.at[i, src_span], (me, partner)
            )
            copy.start()
            waits.append(copy.wait_send)
    for d in range(1, n_sp):
        src_span = at.span_back(d)
        for i, partner in enumerate(at.partners()):
            landed(
                mix_out.at[src_span, share(lax.rem(partner, at.inner))], fwd_recv.at[i, src_span]
            )
        landed(later_out.at[src_span], back_recv.at[src_span])
    for wait in waits:
        wait()


def gradient_after(reached, decays, mix, n_tp):
    n_sp = reached.shape[0]
    inner = 2 if n_tp % 2 == 0 else 1
    return pl.pallas_call(
        functools.partial(after_kernel, n_sp, n_tp),
        out_shape=(
            jax.ShapeDtypeStruct(reached.shape, BF16),
            jax.ShapeDtypeStruct(mix.shape, BF16),
        ),
        in_specs=whole(3),
        out_specs=tuple(whole(2)),
        scratch_shapes=[
            pltpu.VMEM(reached.shape, BF16),
            pltpu.VMEM(reached.shape, BF16),
            DMA((n_sp,)),
            DMA((n_sp,)),
            DMA((n_sp,)),
            DMA((n_sp,)),
            DMA((n_sp,)),
            DMA((n_sp,)),
            DMA((max(inner - 1, 1), n_sp)),
            DMA((max(inner - 1, 1), n_sp)),
        ],
        compiler_params=pltpu.CompilerParams(collective_id=3, has_side_effects=True),
        cost_estimate=pl.CostEstimate(
            flops=15_000_000_000, bytes_accessed=4_000_000, transcendentals=0
        ),
        name="gradient_after",
    )(reached, decays, mix)


def pack_state(state, decay, count):
    width = state.shape[-1]
    per = state.shape[0] * state.shape[1] // count
    row_decay = jnp.repeat(decay, state.shape[1]).reshape(count, per)
    lines = -(-per // width)
    row_decay = jnp.pad(row_decay, ((0, 0), (0, lines * width - per)))
    return jnp.concatenate(
        [state.reshape(count, per, width), row_decay.reshape(count, lines, width)], axis=1
    ).astype(BF16)


HIGHEST = lax.Precision.HIGHEST


def mm(x, y, xd=1, yd=0, precision=None):
    return lax.dot_general(
        x, y, (((xd,), (yd,)), ((), ())), precision=precision, preferred_element_type=F32
    )


def lower_ones(size):
    down = lax.broadcasted_iota(jnp.int32, (size, size), 0)
    across = lax.broadcasted_iota(jnp.int32, (size, size), 1)
    return down >= across


def head_ones(heads, channels):
    down = lax.broadcasted_iota(jnp.int32, (heads, channels), 0)
    across = lax.broadcasted_iota(jnp.int32, (heads, channels), 1)
    return jnp.where(lax.div(across, HDIM) == down, 1.0, 0.0).astype(F32)


def log_decay_sums(step_ref, rate_ref, extra_ref):
    log_decay = extra_ref[...] - step_ref[...] * rate_ref[...]
    lower = jnp.where(lower_ones(log_decay.shape[0]), 1.0, 0.0).astype(F32)
    down = mm(lower, log_decay, precision=HIGHEST)
    across = mm(log_decay, lower, 0, 1, precision=HIGHEST)
    return down, across


def head_decay(down, across, head, mask):
    gap = down[:, head : head + 1] - across[head : head + 1, :]
    return jnp.where(mask, jnp.exp(jnp.where(mask, gap, 0.0)), 0.0)


def group_inverse(gated, group, width):
    part = gated[:, group * width : (group + 1) * width]
    return lax.rsqrt(jnp.mean(part * part, axis=1, keepdims=True) + norm_eps)


def forward_kernel(
    x_ref, step_ref, rate_ref, extra_ref, b_ref, c_ref, before_ref, z_ref, scale_ref, y_ref, norm_ref
):
    tokens, channels = x_ref.shape
    heads = step_ref.shape[1]
    groups = b_ref.shape[1] // STATE
    width = channels // groups
    down, across = log_decay_sums(step_ref, rate_ref, extra_ref)
    wide = head_ones(heads, channels)
    mask = lower_ones(tokens)
    lane = lax.broadcasted_iota(jnp.int32, (tokens, 2 * HDIM), 1)
    scaled = (x_ref[...].astype(F32) * mm(step_ref[...], wide, precision=HIGHEST)).astype(BF16)
    grown = jnp.exp(mm(down, wide, precision=HIGHEST))
    for g in range(groups):
        b_rows = b_ref[:, g * STATE : (g + 1) * STATE]
        c_rows = c_ref[:, g * STATE : (g + 1) * STATE]
        affinity = mm(c_rows, b_rows, 1, 1)
        lanes = slice(g * width, (g + 1) * width)
        off = mm(c_rows, before_ref[lanes], 1, 1) * grown[:, lanes]
        pieces = []
        for pair in range(width // (2 * HDIM)):
            first = g * width + pair * 2 * HDIM
            head = first // HDIM
            values = scaled[:, first : first + 2 * HDIM]
            left = mm((affinity * head_decay(down, across, head, mask)).astype(BF16), values)
            right = mm((affinity * head_decay(down, across, head + 1, mask)).astype(BF16), values)
            pieces.append(jnp.where(lane < HDIM, left, right))
        y = jnp.concatenate(pieces, axis=1) + off
        y_ref[:, lanes] = y
        z = z_ref[:, lanes].astype(F32)
        gated = y * (z * jax.nn.sigmoid(z))
        inverse = group_inverse(gated, 0, width)
        normed = gated * inverse * scale_ref[:, lanes]
        norm_ref[lanes] = normed.T.astype(BF16)


def scan_forward(x, step, rate, extra, b_rows, c_rows, before, gate, scale):
    tokens, channels = x.shape
    return pl.pallas_call(
        forward_kernel,
        out_shape=(
            jax.ShapeDtypeStruct((tokens, channels), F32),
            jax.ShapeDtypeStruct((channels, tokens), BF16),
        ),
        in_specs=whole(9),
        out_specs=tuple(whole(2)),
        cost_estimate=pl.CostEstimate(
            flops=3_000_000_000, bytes_accessed=2_000_000, transcendentals=500_000
        ),
        name="scan_forward",
    )(x, step, rate, extra, b_rows, c_rows, before, gate, scale)


def ring_of(count):
    return [k for k in range(0, count, 2)] + [k for k in reversed(range(1, count, 2))]


def ring_origin(position, count):
    position = lax.rem(position + 2 * count, count)
    return jnp.where(2 * position < count, 2 * position, 2 * count - 1 - 2 * position)


def ring_position(me, count):
    half = lax.div(me, 2)
    return jnp.where(lax.rem(me, 2) == 0, half, count - 1 - half)


class Ring:
    def __init__(self, block):
        self.count = lax.axis_size("sp")
        order = ring_of(self.count)
        self.ahead = [(order[i], order[(i + 1) % self.count]) for i in range(self.count)]
        self.back = [(b, a) for a, b in self.ahead]
        self.blocks, self.shifts = [block], [0]
        self.front = self.rear = block
        self.steps = 0

    def more(self):
        return len(self.blocks) < self.count

    def held(self):
        return (self.front, self.rear)

    def advance(self, held):
        self.front, self.rear = held
        if self.steps:
            self.blocks[self.last[0]] = self.front
            if self.last[1] is not None:
                self.blocks[self.last[1]] = self.rear
        else:
            self.blocks[0] = self.front
        if not self.more():
            return
        self.steps += 1
        self.front = lax.ppermute(self.front, "sp", self.ahead)
        self.blocks.append(self.front)
        self.shifts.append(-self.steps)
        self.last = [len(self.blocks) - 1, None]
        if self.more():
            self.rear = lax.ppermute(self.rear, "sp", self.back)
            self.blocks.append(self.rear)
            self.shifts.append(self.steps)
            self.last[1] = len(self.blocks) - 1


def turn(rings, *values):
    held = [ring.held() for ring in rings]
    values, held = lax.optimization_barrier((values, held))
    for ring, now in zip(rings, held):
        ring.advance(now)
    return values if len(values) > 1 else values[0]


def finish(ring, *values):
    values = turn([ring], *values)
    while ring.more():
        values = turn([ring], *(values if isinstance(values, tuple) else (values,)))
    return values


def norm_grad_kernel(
    n_sp,
    shifts,
    mix_ref,
    y_ref,
    z_ref,
    scale_ref,
    step_ref,
    rate_ref,
    extra_ref,
    c_ref,
    *rest,
):
    weights, (g_ref, gate_ref, reached_ref, total) = rest[:n_sp], rest[n_sp:]
    channels = y_ref.shape[1]
    heads = step_ref.shape[1]
    groups = c_ref.shape[1] // STATE
    width = channels // groups
    position = ring_position(lax.axis_index("sp"), n_sp)
    total[...] = mm(mix_ref[ring_origin(position, n_sp)], weights[0][...], 1, 1)
    for shift, weight in zip(shifts[1:], weights[1:]):
        total[...] += mm(mix_ref[ring_origin(position + shift, n_sp)], weight[...], 1, 1)
    down, _ = log_decay_sums(step_ref, rate_ref, extra_ref)
    grown = jnp.exp(mm(down, head_ones(heads, channels), precision=HIGHEST))
    for g in range(groups):
        lanes = slice(g * width, (g + 1) * width)
        y, z = y_ref[:, lanes], z_ref[:, lanes].astype(F32)
        gate = jax.nn.sigmoid(z)
        silu = z * gate
        gated = y * silu
        inverse = group_inverse(gated, 0, width)
        unit = gated * inverse
        grad = total[:, lanes] * scale_ref[:, lanes]
        grad = inverse * (grad - unit * jnp.mean(grad * unit, axis=1, keepdims=True))
        gate_ref[:, lanes] = (grad * y * gate * (1.0 + z * (1.0 - gate))).astype(BF16)
        scan_grad = grad * silu
        g_ref[:, lanes] = scan_grad
        weighted = (scan_grad * grown[:, lanes]).astype(BF16)
        reached_ref[lanes] = mm(weighted, c_ref[:, g * STATE : (g + 1) * STATE], 0, 0).astype(BF16)


def norm_grad(mix, y, gate, scale, step, rate, extra, c_rows, ring):
    n_sp = mix.shape[0]
    tokens, channels = y.shape
    return pl.pallas_call(
        functools.partial(norm_grad_kernel, n_sp, tuple(ring.shifts)),
        out_shape=(
            jax.ShapeDtypeStruct((tokens, channels), F32),
            jax.ShapeDtypeStruct((tokens, channels), BF16),
            jax.ShapeDtypeStruct((channels, STATE), BF16),
        ),
        in_specs=whole(8 + n_sp),
        out_specs=tuple(whole(3)),
        scratch_shapes=[pltpu.VMEM((tokens, channels), F32)],
        cost_estimate=pl.CostEstimate(
            flops=4_000_000_000, bytes_accessed=6_000_000, transcendentals=500_000
        ),
        name="norm_grad",
    )(mix, y, gate, scale, step, rate, extra, c_rows, *ring.blocks)


def backward_kernel(
    x_ref,
    step_ref,
    rate_ref,
    extra_ref,
    b_ref,
    c_ref,
    before_ref,
    g_ref,
    later_ref,
    dx_ref,
    dstep_ref,
    db_ref,
    dc_ref,
):
    tokens, channels = x_ref.shape
    heads = step_ref.shape[1]
    groups = b_ref.shape[1] // STATE
    width = channels // groups
    down, across = log_decay_sums(step_ref, rate_ref, extra_ref)
    wide = head_ones(heads, channels)
    mask = lower_ones(tokens)
    lane = lax.broadcasted_iota(jnp.int32, (tokens, 2 * HDIM), 1)
    head_lane = lax.broadcasted_iota(jnp.int32, (tokens, heads), 1)
    head_down = lax.broadcasted_iota(jnp.int32, (heads, tokens), 0)
    last = down[tokens - 1 : tokens, :]
    step_wide = mm(step_ref[...], wide, precision=HIGHEST)
    down_wide = mm(down, wide, precision=HIGHEST)
    grown = jnp.exp(down_wide)
    to_end = jnp.exp(down_wide[tokens - 1 : tokens, :] - down_wide)
    x = x_ref[...].astype(F32)
    scaled = x * step_wide
    scaled_low = scaled.astype(BF16)
    sums = jnp.zeros((tokens, heads), F32)
    column_sums = jnp.zeros((heads, tokens), F32)
    through = []
    ended = []
    stepped = []
    carried = []
    for g in range(groups):
        lanes = slice(g * width, (g + 1) * width)
        states = slice(g * STATE, (g + 1) * STATE)
        b_rows, c_rows = b_ref[:, states], c_ref[:, states]
        affinity = mm(c_rows, b_rows, 1, 1)
        before, later = before_ref[lanes], later_ref[lanes]
        grad = g_ref[:, lanes]
        grad_low = grad.astype(BF16)
        affinity_grad = jnp.zeros((tokens, tokens), F32)
        pieces = []
        for pair in range(width // (2 * HDIM)):
            start = pair * 2 * HDIM
            values = scaled_low[:, g * width + start : g * width + start + 2 * HDIM]
            grads = grad_low[:, start : start + 2 * HDIM]
            halves = []
            for side in range(2):
                head = (g * width + start) // HDIM + side
                decay = head_decay(down, across, head, mask)
                own = grads * jnp.where((lane < HDIM) == (side == 0), 1.0, 0.0).astype(BF16)
                inner = mm(own, values, 1, 1) * decay
                affinity_grad = affinity_grad + inner
                moved = inner * affinity
                sums = sums + jnp.where(
                    head_lane == head, jnp.sum(moved, axis=1, keepdims=True), 0.0
                )
                column_sums = column_sums + jnp.where(
                    head_down == head, jnp.sum(moved, axis=0, keepdims=True), 0.0
                )
                halves.append(mm((affinity * decay).astype(BF16), grads, 0, 0))
            pieces.append(jnp.where(lane < HDIM, halves[0], halves[1]))
        ends = to_end[:, lanes]
        from_later = mm(b_rows, later, 1, 1) * ends
        scaled_grad = jnp.concatenate(pieces, axis=1) + from_later
        off = mm(c_rows, before, 1, 1) * grown[:, lanes]
        through.append(grad * off)
        ended.append(scaled[:, lanes] * from_later)
        stepped.append(scaled_grad * x[:, lanes])
        dx_ref[:, lanes] = (scaled_grad * step_wide[:, lanes]).astype(BF16)
        low = affinity_grad.astype(BF16)
        dc_ref[:, states] = (
            mm(low, b_rows) + mm((grad * grown[:, lanes]).astype(BF16), before)
        ).astype(BF16)
        db_ref[:, states] = (
            mm(low, c_rows, 0, 0) + mm((scaled[:, lanes] * ends).astype(BF16), later)
        ).astype(BF16)
        both = jnp.sum(before.astype(F32) * later.astype(F32), axis=1, keepdims=True)
        carried.append(both)
    through = mm(jnp.concatenate(through, axis=1), wide, 1, 1, precision=HIGHEST)
    ended = mm(jnp.concatenate(ended, axis=1), wide, 1, 1, precision=HIGHEST)
    stepped = mm(jnp.concatenate(stepped, axis=1), wide, 1, 1, precision=HIGHEST)
    both = jnp.broadcast_to(jnp.concatenate(carried, axis=0), (channels, STATE))
    carried = mm(jnp.ones((8, STATE), F32), mm(wide, both, precision=HIGHEST), 1, 1, HIGHEST)
    carried = carried[:1] * (1.0 / STATE) * jnp.exp(last)
    moved = sums - column_sums.T + through - ended
    final = jnp.sum(ended, axis=0, keepdims=True) + carried
    lower = jnp.where(mask, 1.0, 0.0).astype(F32)
    decay_grad = mm(lower, moved, 0, 0, precision=HIGHEST) + final
    dstep_ref[...] = stepped - rate_ref[...] * decay_grad


def scan_backward(x, step, rate, extra, b_rows, c_rows, before, grad, later):
    tokens, channels = x.shape
    return pl.pallas_call(
        backward_kernel,
        out_shape=(
            jax.ShapeDtypeStruct(x.shape, BF16),
            jax.ShapeDtypeStruct(step.shape, F32),
            jax.ShapeDtypeStruct(b_rows.shape, BF16),
            jax.ShapeDtypeStruct(c_rows.shape, BF16),
        ),
        in_specs=whole(9),
        out_specs=tuple(whole(4)),
        cost_estimate=pl.CostEstimate(
            flops=5_000_000_000, bytes_accessed=3_000_000, transcendentals=500_000
        ),
        name="scan_backward",
    )(x, step, rate, extra, b_rows, c_rows, before, grad, later)


def projection_kernel(n_sp, shifts, mix_ref, *rest):
    blocks, out_ref = rest[:n_sp], rest[n_sp]
    position = ring_position(lax.axis_index("sp"), n_sp)
    out_ref[...] = mm(blocks[0][...], mix_ref[ring_origin(position, n_sp)])
    for shift, block in zip(shifts[1:], blocks[1:]):
        out_ref[...] += mm(block[...], mix_ref[ring_origin(position + shift, n_sp)])


def projection_grad(mix_columns, ring):
    n_sp, _, columns = mix_columns.shape
    channels = ring.blocks[0].shape[0]
    return pl.pallas_call(
        functools.partial(projection_kernel, n_sp, tuple(ring.shifts)),
        out_shape=jax.ShapeDtypeStruct((channels, columns), F32),
        in_specs=whole(1 + n_sp),
        out_specs=whole(1)[0],
        cost_estimate=pl.CostEstimate(
            flops=3_000_000_000, bytes_accessed=3_000_000, transcendentals=0
        ),
        name="projection_grad",
    )(mix_columns, *ring.blocks)


def weight_grad_kernel(rows_ref, gate_ref, up_ref, hidden_ref, sent_ref, g_out, u_out, d_out):
    g_out[...] = mm(rows_ref[...], gate_ref[...], 0, 0).astype(BF16)
    u_out[...] = mm(rows_ref[...], up_ref[...], 0, 0).astype(BF16)
    d_out[...] = mm(hidden_ref[...], sent_ref[...], 0, 0).astype(BF16)


def expert_weight_grads(routed_rows, routed_grads, hidden, gate_grad, up_grad):
    pairs, model_width = routed_rows.shape
    units = hidden.shape[1]
    tile = 256
    across = pl.BlockSpec((pairs, tile), lambda i: (0, i))
    fixed = pl.BlockSpec((pairs, units), lambda i: (0, 0))
    tall = pl.BlockSpec((tile, units), lambda i: (i, 0))
    return pl.pallas_call(
        weight_grad_kernel,
        grid=(model_width // tile,),
        out_shape=(
            jax.ShapeDtypeStruct((model_width, units), BF16),
            jax.ShapeDtypeStruct((model_width, units), BF16),
            jax.ShapeDtypeStruct((units, model_width), BF16),
        ),
        in_specs=[across, fixed, fixed, fixed, across],
        out_specs=(tall, tall, pl.BlockSpec((units, tile), lambda i: (0, i))),
        cost_estimate=pl.CostEstimate(
            flops=6_000_000_000, bytes_accessed=16_000_000, transcendentals=0
        ),
        name="expert_weight_grads",
    )(routed_rows, gate_grad, up_grad, hidden, routed_grads)


def span_final_state(input_heads, time_step, decay_speed, sudden_decay, input_vector_groups):
    length, head_count, head_size = input_heads.shape
    groups = input_vector_groups.shape[1]
    log_decay_total = sudden_decay - time_step * decay_speed[None, :]
    sum_total = jnp.sum(log_decay_total, axis=0)
    after = sum_total[None, :] - jnp.cumsum(log_decay_total, axis=0)
    weighted = (input_heads * (time_step * jnp.exp(after))[:, :, None]).reshape(
        length, groups, head_count // groups, head_size
    )
    result = jnp.einsum("tgn,tghp->ghpn", input_vector_groups, weighted, precision=exact_mode)
    return (result.reshape(head_count, head_size, -1), jnp.exp(sum_total))


def slot_choice(route_rows, expert_count, capacity):
    flat_routes = route_rows.reshape(-1)
    pairs = flat_routes.shape[0]
    onehot = flat_routes[:, None] == jnp.arange(expert_count, dtype=jnp.int32)[None, :]
    earlier = jnp.tril(jnp.ones((pairs, pairs), jnp.bfloat16), -1)
    before = jnp.dot(earlier, onehot.astype(jnp.bfloat16), preferred_element_type=jnp.float32)
    place = jnp.sum(jnp.where(onehot, before, 0.0), axis=1).astype(jnp.int32)
    destination = (flat_routes * capacity + place).reshape(route_rows.shape)
    slots = jnp.arange(expert_count * capacity, dtype=jnp.int32)
    return [slots[:, None] == destination[None, :, k] for k in range(route_rows.shape[1])]


def pack_rows(stream, grad_rows, chosen, weights):
    pick = sum(c.astype(jnp.bfloat16) for c in chosen)
    weight_of = sum(
        jnp.sum(jnp.where(c, weights[None, :, k], 0.0), axis=1) for k, c in enumerate(chosen)
    )
    routed = jnp.dot(pick, stream, preferred_element_type=jnp.float32).astype(jnp.bfloat16)
    picked = jnp.dot(pick, grad_rows, preferred_element_type=jnp.float32)
    return (routed, (picked * weight_of[:, None]).astype(jnp.bfloat16), pick)


def expert_hidden(routed_rows, routed_grads, w_gate, w_up, w_down):
    pre_gate = jnp.dot(routed_rows, w_gate, preferred_element_type=jnp.float32)
    pre_up = jnp.dot(routed_rows, w_up, preferred_element_type=jnp.float32)
    activated = jax.nn.silu(pre_gate)
    hidden = (activated * pre_up).astype(jnp.bfloat16)
    hidden_grad = lax.dot_general(
        routed_grads, w_down, (((1,), (1,)), ((), ())), preferred_element_type=jnp.float32
    )
    sigmoid_gate = jax.nn.sigmoid(pre_gate)
    gate_grad = (
        hidden_grad * pre_up * sigmoid_gate * (1.0 + pre_gate * (1.0 - sigmoid_gate))
    ).astype(jnp.bfloat16)
    up_grad = (hidden_grad * activated).astype(jnp.bfloat16)
    return (hidden, gate_grad, up_grad)


def row_partial(gate_grad, up_grad, w_gate, w_up):
    contract = (((1,), (1,)), ((), ()))
    partial_sum = lax.dot_general(gate_grad, w_gate, contract, preferred_element_type=jnp.float32)
    partial_sum = partial_sum + lax.dot_general(
        up_grad, w_up, contract, preferred_element_type=jnp.float32
    )
    return lax.optimization_barrier(partial_sum.astype(jnp.bfloat16)).astype(jnp.float32)


def body(
    mixer_output_stream,
    layer_output_gradient,
    routes,
    expert_combine_weight,
    expert_gate_weight,
    expert_up_weight,
    expert_down_weight,
    head_mixer_input,
    head_step_size,
    head_decay_rate,
    extra_log_decay,
    state_entering_span,
    state_input_vectors,
    state_readout_vectors,
    gate_preactivation,
    group_norm_scale,
    mixer_output_weight,
):
    expert_count = lax.axis_size("sp")
    local_tokens = routes.shape[0]
    capacity = 3 * local_tokens // expert_count
    chosen = slot_choice(routes, expert_count, capacity)
    w_gate = expert_gate_weight[0]
    w_up = expert_up_weight[0]
    w_down = expert_down_weight[0]
    sent_rows, sent_grads, pick = pack_rows(
        mixer_output_stream, layer_output_gradient, chosen, expert_combine_weight
    )
    n_tp = lax.axis_size("tp")
    head_local = head_step_size.shape[1]
    group_local = state_input_vectors.shape[1] // STATE
    input_heads = head_mixer_input.astype(jnp.float32).reshape(local_tokens, head_local, HDIM)
    input_vector_groups = state_input_vectors.astype(jnp.float32).reshape(
        local_tokens, group_local, STATE
    )
    within_span_state, within_span_decay = span_final_state(
        input_heads, head_step_size, head_decay_rate, extra_log_decay, input_vector_groups
    )
    state_rows = head_local * HDIM
    per_span = state_rows // expert_count
    first_rows = lax.dynamic_slice_in_dim(
        state_entering_span.reshape(state_rows, STATE), lax.axis_index("sp") * per_span, per_span, 0
    )
    packed_state = pack_state(within_span_state, within_span_decay, expert_count)
    weight_ring = Ring(mixer_output_weight)
    weight_ring.advance(weight_ring.held())
    routed_rows, routed_grads, arrived_state = dispatch(
        sent_rows.reshape(expert_count, capacity, -1),
        sent_grads.reshape(expert_count, capacity, -1),
        packed_state,
        n_tp,
    )
    routed_rows, routed_grads, arrived_state = turn(
        [weight_ring], routed_rows, routed_grads, arrived_state
    )
    model_width = routed_rows.shape[2]
    routed_rows = routed_rows.reshape(-1, model_width)
    routed_grads = routed_grads.reshape(-1, model_width)
    hidden, gate_grad, up_grad = expert_hidden(routed_rows, routed_grads, w_gate, w_up, w_down)
    partial_rows = row_partial(gate_grad, up_grad, w_gate, w_up)
    partial_rows = partial_rows.astype(jnp.bfloat16).reshape(expert_count, capacity, model_width)
    partial_rows, arrived_state = turn([weight_ring], partial_rows, arrived_state)
    mix_grad, before, span_decays = return_rows(
        partial_rows,
        layer_output_gradient,
        pick.reshape(expert_count, capacity, local_tokens).swapaxes(1, 2),
        arrived_state,
        first_rows,
        n_tp,
    )
    mix_grad, before, hidden, gate_grad, up_grad = turn(
        [weight_ring], mix_grad, before, hidden, gate_grad, up_grad
    )
    rate = head_decay_rate[None, :]
    scale = group_norm_scale[None, :]
    before_rows = before.reshape(state_rows, STATE)
    scan_out, normed = scan_forward(
        head_mixer_input,
        head_step_size,
        rate,
        extra_log_decay,
        state_input_vectors,
        state_readout_vectors,
        before_rows,
        gate_preactivation,
        scale,
    )
    grad_g, grad_u, grad_d = expert_weight_grads(
        routed_rows, routed_grads, hidden, gate_grad, up_grad
    )
    mix_parts = mix_grad.reshape(local_tokens, expert_count, -1).swapaxes(0, 1)
    scan_out, normed, mix_parts, grad_d = finish(
        weight_ring, scan_out, normed, mix_parts, grad_d
    )
    normed_ring = Ring(normed)
    normed_ring.advance(normed_ring.held())
    scan_grad, gate_grad_in, reached = norm_grad(
        mix_parts,
        scan_out,
        gate_preactivation,
        scale,
        head_step_size,
        rate,
        extra_log_decay,
        state_readout_vectors,
        weight_ring,
    )
    scan_grad, reached = turn([normed_ring], scan_grad, reached)
    later_grad, mix_columns = gradient_after(
        reached.reshape(before.shape), span_decays, mix_parts, n_tp
    )
    later_grad, mix_columns = turn([normed_ring], later_grad, mix_columns)
    input_grad, step_grad, b_grad, c_grad = scan_backward(
        head_mixer_input,
        head_step_size,
        rate,
        extra_log_decay,
        state_input_vectors,
        state_readout_vectors,
        before_rows,
        scan_grad,
        later_grad.reshape(state_rows, STATE),
    )
    input_grad, mix_columns = finish(normed_ring, input_grad, mix_columns)
    proj_grad = projection_grad(mix_columns, normed_ring)
    return (
        grad_g[None],
        grad_u[None],
        grad_d[None],
        proj_grad,
        input_grad,
        step_grad,
        b_grad,
        c_grad,
        gate_grad_in,
    )


def solution(mesh):
    return jax.shard_map(
        body,
        mesh=mesh,
        in_specs=(
            P("sp", "tp"),
            P("sp", "tp"),
            P("sp", None),
            P("sp", None),
            P("sp", None, "tp"),
            P("sp", None, "tp"),
            P("sp", "tp", None),
            P("sp", "tp"),
            P("sp", "tp"),
            P("tp"),
            P("sp", "tp"),
            P("tp", None, None),
            P("sp", "tp"),
            P("sp", "tp"),
            P("sp", "tp"),
            P("tp"),
            P("tp", "sp"),
        ),
        out_specs=(
            P("sp", None, "tp"),
            P("sp", None, "tp"),
            P("sp", "tp", None),
            P("tp", "sp"),
            P("sp", "tp"),
            P("sp", "tp"),
            P("sp", "tp"),
            P("sp", "tp"),
            P("sp", "tp"),
        ),
        check_vma=False,
    )
```

```python
import functools

import jax
import jax.numpy as jnp
from jax import lax
from jax.experimental import pallas as pl
from jax.experimental.pallas import tpu as pltpu
from jax.sharding import PartitionSpec as P

HDIM = 64
STATE = 128
BLK = 128


norm_eps = 1e-05
exact_mode = lax.Precision.HIGH


MESH = pl.DeviceIdType.MESH
BF16 = jnp.bfloat16
F32 = jnp.float32
DMA = pltpu.SemaphoreType.DMA


class Place:
    def __init__(self, n_sp, n_tp):
        self.n_sp, self.n_tp = n_sp, n_tp
        self.inner = 2 if n_tp % 2 == 0 else 1
        self.outer = n_tp // self.inner
        self.me = lax.axis_index("sp")
        self.t = lax.axis_index("tp")
        self.core = lax.rem(self.t, self.inner)
        self.far = lax.div(self.t, self.inner)

    def span(self, d):
        return lax.rem(self.me + d, self.n_sp)

    def span_back(self, d):
        return lax.rem(self.me + (self.n_sp - d), self.n_sp)

    def partners(self):
        return [self.far * self.inner + lax.rem(self.core + i, self.inner) for i in range(1, self.inner)]

    def outers(self):
        return [lax.rem(self.far + j, self.outer) * self.inner + self.core for j in range(1, self.outer)]

    def enter(self, with_span=True):
        barrier = pltpu.get_barrier_semaphore()
        devices = [(self.me, p) for p in self.partners() + self.outers()]
        if with_span:
            devices += [(self.span(d), self.t) for d in range(1, self.n_sp)]
        for device in devices:
            pl.semaphore_signal(barrier, inc=1, device_id=device, device_id_type=MESH)
        pl.semaphore_wait(barrier, len(devices))


def remote(src, dst, send, recv, device):
    return pltpu.make_async_remote_copy(
        src_ref=src, dst_ref=dst, send_sem=send, recv_sem=recv, device_id=device, device_id_type=MESH
    )


def decay_column(row, per):
    width = row.shape[-1]
    down = lax.broadcasted_iota(jnp.int32, (per, width), 0)
    across = lax.broadcasted_iota(jnp.int32, (per, width), 1)
    spread = jnp.broadcast_to(row.astype(F32), (per, width))
    return jnp.sum(jnp.where(down == across, spread, 0.0), axis=1, keepdims=True)


def whole(count):
    return [pl.BlockSpec(memory_space=pltpu.VMEM)] * count


HIGHEST = lax.Precision.HIGHEST


def mm(x, y, xd=1, yd=0, precision=None):
    return lax.dot_general(
        x, y, (((xd,), (yd,)), ((), ())), precision=precision, preferred_element_type=F32
    )


def lower_ones(size):
    down = lax.broadcasted_iota(jnp.int32, (size, size), 0)
    across = lax.broadcasted_iota(jnp.int32, (size, size), 1)
    return down >= across


def head_ones(heads, channels):
    down = lax.broadcasted_iota(jnp.int32, (heads, channels), 0)
    across = lax.broadcasted_iota(jnp.int32, (heads, channels), 1)
    return jnp.where(lax.div(across, HDIM) == down, 1.0, 0.0).astype(F32)


def turned(x):
    size = x.shape[1]
    down = lax.broadcasted_iota(jnp.int32, (size, size), 0)
    across = lax.broadcasted_iota(jnp.int32, (size, size), 1)
    return mm(jnp.where(down == across, 1.0, 0.0).astype(F32), x, 1, 1, HIGHEST)


def log_decay_sums(step_ref, rate_ref, extra_ref):
    heads, tokens = step_ref.shape
    log_decay = extra_ref[...] - step_ref[...] * decay_column(rate_ref[...], heads)
    lower = jnp.where(lower_ones(tokens), 1.0, 0.0).astype(F32)
    down = mm(lower, log_decay, 1, 1, HIGHEST)
    across = mm(log_decay, lower, 1, 1, HIGHEST)
    return down, across


def head_decay(down, across, head, mask):
    gap = down[:, head : head + 1] - across[head : head + 1, :]
    return jnp.where(mask, jnp.exp(jnp.where(mask, gap, 0.0)), 0.0)


def group_inverse(gated, group, width):
    part = gated[:, group * width : (group + 1) * width]
    return lax.rsqrt(jnp.mean(part * part, axis=1, keepdims=True) + norm_eps)


def ring_origin(position, count):
    position = lax.rem(position + 2 * count, count)
    return jnp.where(2 * position < count, 2 * position, 2 * count - 1 - 2 * position)


def ring_position(me, count):
    half = lax.div(me, 2)
    return jnp.where(lax.rem(me, 2) == 0, half, count - 1 - half)


class Circle:
    def __init__(self, at, own, slots, sends, recvs, waits):
        self.at, self.own, self.slots = at, own, slots
        self.sends, self.recvs, self.waits = sends, recvs, waits
        self.half = at.n_sp // 2
        self.position = ring_position(at.me, at.n_sp)
        self.after = ring_origin(self.position + 1, at.n_sp)
        self.prior = ring_origin(self.position - 1, at.n_sp)
        self.step = 0

    def block(self, slot):
        return self.own if slot == 0 else self.slots.at[slot]

    def origin(self, slot):
        shift = -slot if slot <= self.half else slot - self.half
        return ring_origin(self.position + shift, self.at.n_sp)

    def part(self, block, p):
        size = self.own.shape[0] // 2
        return block.at[pl.ds(p * size, size)]

    def send(self, source, slot, p, peer):
        copy = remote(
            self.part(source, p),
            self.part(self.slots.at[slot], p),
            self.sends.at[slot, p],
            self.recvs.at[slot, p],
            (peer, self.at.t),
        )
        copy.start()
        self.waits.append(copy.wait_send)

    def landed(self, slot, p):
        block = self.part(self.slots.at[slot], p)
        pltpu.make_async_copy(block, block, self.recvs.at[slot, p]).wait()

    def advance(self):
        half, step = self.half, self.step
        self.step = step + 1
        front, rear = self.block(step), self.block(half + step if step else 0)
        for p in range(2):
            if step and step <= half:
                self.landed(step, p)
            if step and step < half:
                self.landed(half + step, p)
            if step + 1 < half:
                self.send(front, step + 1, p, self.after)
                self.send(rear, half + step + 1, p, self.prior)
            elif step + 1 == half and p == 0:
                self.send(front, half, p, self.after)
            elif step + 1 == half:
                self.send(rear, half, p, self.prior)
        if step == 0:
            return [0]
        return [step, half + step] if step < half else [step]

    def more(self):
        return self.step <= self.half


def main_kernel(
    n_sp,
    n_tp,
    stream_ref,
    own_grad_ref,
    routes_ref,
    combine_ref,
    wg_hbm,
    wu_hbm,
    wd_hbm,
    entering_ref,
    x_ref,
    step_ref,
    rate_ref,
    extra_ref,
    b_ref,
    c_ref,
    z_ref,
    scale_ref,
    out_w_ref,
    rows_t_hbm,
    sent_hbm,
    hidden_t_hbm,
    gate_grad_hbm,
    up_grad_hbm,
    proj_ref,
    dx_ref,
    dstep_ref,
    db_ref,
    dc_ref,
    dgate_ref,
    rows,
    sent,
    rows_t,
    hidden_ref,
    hidden_t,
    gate_grad_ref,
    up_grad_ref,
    rows_out,
    sent_out,
    pick_ref,
    state_out,
    state_in,
    lines_out,
    lines_in,
    span_send,
    tp_send,
    tp_fwd_send,
    block_recv,
    state_send,
    state_recv,
    lines_send,
    lines_recv,
    save_sem,
    wg,
    wu,
    wd,
    acc_gate,
    acc_up,
    acc_down,
    part,
    pair_in,
    far_out,
    far_in,
    ret_out,
    ret_in,
    before_tmp,
    before_in,
    mix_own,
    mix,
    mix_parts,
    mix_cols,
    w_slots,
    norm_own,
    norm_slots,
    y_ref,
    total_ref,
    scaled_ref,
    grown_ref,
    ends_ref,
    g_ref,
    sgrad_ref,
    dbp_ref,
    moved_ref,
    reached_ref,
    reached_in,
    after_tmp,
    later_in,
    load_sem,
    pair_send,
    pair_recv,
    far_send,
    far_recv,
    ret_send,
    ret_recv,
    mix_send,
    mix_recv,
    back_send,
    back_recv,
    w_send,
    w_recv,
    norm_send,
    norm_recv,
    reach_send,
    reach_recv,
    later_send,
    later_recv,
    cols_send,
    near_send,
    fwd_send,
    cols_recv,
):
    at = Place(n_sp, n_tp)
    me, t = at.me, at.t
    width = own_grad_ref.shape[1]
    _, capacity, model_width = rows.shape
    pairs = n_sp * capacity
    tokens, channels = x_ref.shape
    per = channels // n_sp
    heads = step_ref.shape[0]
    groups = b_ref.shape[1] // STATE
    group_width = channels // groups
    waits = []

    def cols(owner):
        return pl.ds(pl.multiple_of(owner * width, width), width)

    def landed(block, sem):
        pltpu.make_async_copy(block, block, sem).wait()

    def push(source, target, send, recv, device):
        copy = remote(source, target, send, recv, device)
        copy.start()
        waits.append(copy.wait_send)

    loads = []
    for i, (source, target) in enumerate(((wg_hbm, wg), (wu_hbm, wu), (wd_hbm, wd))):
        loads.append(pltpu.make_async_copy(source, target, load_sem.at[i]))
        loads[-1].start()
    at.enter()
    w_ring = Circle(at, out_w_ref, w_slots, w_send, w_recv, waits)
    norm_ring = Circle(at, norm_own, norm_slots, norm_send, norm_recv, waits)
    w_ring.advance()

    routes = turned(routes_ref[...].astype(F32))
    combine = turned(combine_ref[...])
    top = routes.shape[1]
    expert_lane = lax.broadcasted_iota(jnp.int32, (tokens, n_sp), 1).astype(F32)
    slot_lane = lax.broadcasted_iota(jnp.int32, (tokens, capacity), 1).astype(F32)
    mask = lower_ones(tokens)
    named = [routes[:, k : k + 1] == expert_lane for k in range(top)]
    ones = sum(jnp.where(n, 1.0, 0.0) for n in named)
    earlier = mm(jnp.where(mask, 1.0, 0.0).astype(BF16), ones.astype(BF16)) - ones
    weighted = [
        (own_grad_ref[...].astype(F32) * combine[:, k : k + 1]).astype(BF16) for k in range(top)
    ]
    places = [jnp.sum(jnp.where(n, earlier, 0.0), axis=1, keepdims=True) for n in named]
    for e in range(n_sp):
        picks = []
        for k in range(top):
            place = jnp.where(routes[:, k : k + 1] == float(e), places[k], -1.0)
            picks.append(jnp.where(place == slot_lane, 1.0, 0.0).astype(BF16))
        pick = sum(picks)
        pick_ref[e] = pick
        rows_out[e] = mm(pick, stream_ref[...], 0, 0).astype(BF16)
        sent_out[e] = sum(mm(p, w, 0, 0) for p, w in zip(picks, weighted)).astype(BF16)
    both = ((rows_out, rows), (sent_out, sent))
    for d in range(1, n_sp):
        peer = at.span(d)
        for a, (source, target) in enumerate(both):
            push(
                source.at[peer],
                target.at[me, :, cols(t)],
                span_send.at[a, d],
                block_recv.at[a, me, t],
                (peer, t),
            )

    def pass_on(d, sources, peers, owner, sems, base):
        src_span = at.span_back(d)
        for a in range(2):
            for i, peer in enumerate(peers):
                push(
                    sources[a],
                    both[a][1].at[src_span, :, cols(owner)],
                    sems.at[a, d, base + i],
                    block_recv.at[a, src_span, owner],
                    (me, peer),
                )

    def block_landed(a, src_span, owner):
        landed(both[a][1].at[src_span, :, cols(owner)], block_recv.at[a, src_span, owner])

    near = at.outers() + at.partners()
    pass_on(0, [rows_out.at[me], sent_out.at[me]], near, t, tp_send, 0)
    rows[me, :, cols(t)] = rows_out[me]
    sent[me, :, cols(t)] = sent_out[me]

    down, across = log_decay_sums(step_ref, rate_ref, extra_ref)
    wide = head_ones(heads, channels)
    lane = lax.broadcasted_iota(jnp.int32, (tokens, 2 * HDIM), 1)
    step_wide = mm(turned(step_ref[...]), wide, precision=HIGHEST)
    scaled_ref[...] = x_ref[...].astype(F32) * step_wide
    down_wide = mm(down, wide, precision=HIGHEST)
    grown_ref[...] = jnp.exp(down_wide)
    ends_ref[...] = jnp.exp(down_wide[tokens - 1 : tokens, :] - down_wide)
    spans = n_sp // groups
    for g in range(groups):
        lanes = slice(g * group_width, (g + 1) * group_width)
        left = (scaled_ref[:, lanes] * ends_ref[:, lanes]).astype(BF16)
        state = mm(left, b_ref[:, g * STATE : (g + 1) * STATE], 0, 0).astype(BF16)
        state_out[g * spans : (g + 1) * spans] = state.reshape(spans, per, STATE)
    whole_decay = jnp.exp(down_wide[tokens - 1 : tokens, :])
    lines_out[...] = jnp.zeros(lines_out.shape, BF16)
    for k in range(n_sp):
        lines_out[k, :, :per] = whole_decay[:, k * per : (k + 1) * per].astype(BF16)
    for d in range(1, n_sp):
        peer = at.span(d)
        push(state_out.at[peer], state_in.at[me], state_send.at[d], state_recv.at[me], (peer, t))
        push(lines_out.at[peer], lines_in.at[me], lines_send.at[d], lines_recv.at[me], (peer, t))
    state_in[me] = state_out[me]
    lines_in[me] = lines_out[me]

    for d in range(1, n_sp):
        src_span = at.span_back(d)
        for a in range(2):
            block_landed(a, src_span, t)
        pass_on(d, [b[1].at[src_span, :, cols(t)] for b in both], near, t, tp_send, 0)
    for d in range(n_sp):
        src_span = at.span_back(d)
        for j, owner in enumerate(at.outers()):
            for a in range(2):
                block_landed(a, src_span, owner)
            pass_on(
                d,
                [b[1].at[src_span, :, cols(owner)] for b in both],
                at.partners(),
                owner,
                tp_fwd_send,
                j * (at.inner - 1),
            )
    for d in range(1, n_sp):
        src_span = at.span_back(d)
        landed(state_in.at[src_span], state_recv.at[src_span])
        landed(lines_in.at[src_span], lines_recv.at[src_span])
    running = entering_ref[pl.ds(pl.multiple_of(me * per, per), per), :]
    for k in range(n_sp):
        before_tmp[k] = running.astype(BF16)
        running = decay_column(lines_in[k], per) * running + state_in[k].astype(F32)
    for d in range(1, n_sp):
        peer = at.span(d)
        push(before_tmp.at[peer], before_in.at[me], back_send.at[d], back_recv.at[me], (peer, t))
    before_in[me] = before_tmp[me]
    w_there = [0] + w_ring.advance()
    for d in range(n_sp):
        src_span = at.span_back(d)
        for partner in at.partners():
            core = lax.rem(partner, at.inner)
            for far in range(at.outer):
                for a in range(2):
                    block_landed(a, src_span, far * at.inner + core)

    saves = []

    def save(source, target):
        copy = pltpu.make_async_copy(source, target, save_sem.at[len(saves)])
        copy.start()
        saves.append(copy)

    save(sent, sent_hbm)

    deep = 256

    def chunk(i):
        return pl.ds(pl.multiple_of(i * deep, deep), deep)

    acc_gate[...] = jnp.zeros(acc_gate.shape, F32)
    acc_up[...] = jnp.zeros(acc_up.shape, F32)
    acc_down[...] = jnp.zeros(acc_down.shape, F32)
    loads[0].wait()

    @pl.loop(0, model_width // deep)
    def _(i):
        acc_gate[...] += mm(rows[:, :, chunk(i)].reshape(pairs, deep), wg[chunk(i), :])

    loads[1].wait()

    @pl.loop(0, model_width // deep)
    def _(i):
        acc_up[...] += mm(rows[:, :, chunk(i)].reshape(pairs, deep), wu[chunk(i), :])

    loads[2].wait()

    @pl.loop(0, model_width // deep)
    def _(i):
        acc_down[...] += mm(sent[:, :, chunk(i)].reshape(pairs, deep), wd[:, chunk(i)], 1, 1)

    @pl.loop(0, n_sp)
    def _(i):
        piece = pl.ds(pl.multiple_of(i * capacity, capacity), capacity)
        pre_gate, pre_up, hidden_grad = acc_gate[piece, :], acc_up[piece, :], acc_down[piece, :]
        gate = jax.nn.sigmoid(pre_gate)
        silu = pre_gate * gate
        hidden_ref[piece, :] = (silu * pre_up).astype(BF16)
        slope = gate * (1.0 + pre_gate * (1.0 - gate))
        gate_grad_ref[piece, :] = (hidden_grad * pre_up * slope).astype(BF16)
        up_grad_ref[piece, :] = (hidden_grad * silu).astype(BF16)

    order = list(range(1, n_sp)) + [0]
    fars = list(range(1, at.outer)) + [0]

    def partial_columns(owner):
        rows = cols(owner)
        value = mm(gate_grad_ref[...], wg[rows, :], 1, 1) + mm(up_grad_ref[...], wu[rows, :], 1, 1)
        part[:, :, rows] = value.astype(BF16).reshape(n_sp, capacity, width)

    for i, partner in enumerate(at.partners()):
        core = lax.rem(partner, at.inner)
        for j in fars:
            far = lax.rem(at.far + j, at.outer)
            owner = far * at.inner + core
            partial_columns(owner)
            for d in order:
                span = at.span(d)
                push(
                    part.at[span, :, cols(owner)],
                    pair_in.at[i, j, span],
                    pair_send.at[i, j, d],
                    pair_recv.at[i, j, span],
                    (me, partner),
                )
    for j in fars:
        partial_columns(lax.rem(at.far + j, at.outer) * at.inner + at.core)

    def pair_sum(span, j):
        far = lax.rem(at.far + j, at.outer)
        value = part[span, :, cols(far * at.inner + at.core)].astype(F32)
        for i in range(at.inner - 1):
            value = value + pair_in[i, j, span].astype(F32)
        return value

    for d in order:
        span = at.span(d)
        for j in fars:
            for i in range(at.inner - 1):
                landed(pair_in.at[i, j, span], pair_recv.at[i, j, span])
            if j:
                far_out[j - 1, span] = pair_sum(span, j).astype(BF16)
                push(
                    far_out.at[j - 1, span],
                    far_in.at[j - 1, span],
                    far_send.at[j - 1, d],
                    far_recv.at[j - 1, span],
                    (me, lax.rem(at.far + j, at.outer) * at.inner + at.core),
                )
    w_there += w_ring.advance()
    save(gate_grad_ref, gate_grad_hbm)
    save(up_grad_ref, up_grad_hbm)

    for d in range(1, n_sp):
        src_span = at.span_back(d)
        landed(before_in.at[src_span], back_recv.at[src_span])
    before_rows = before_in[...].reshape(n_sp * per, STATE)
    for g in range(groups):
        states = slice(g * STATE, (g + 1) * STATE)
        lanes = slice(g * group_width, (g + 1) * group_width)
        b_rows, c_rows = b_ref[:, states], c_ref[:, states]
        affinity = mm(c_rows, b_rows, 1, 1)
        off = mm(c_rows, before_rows[lanes], 1, 1) * grown_ref[:, lanes]
        pieces = []
        for pair in range(group_width // (2 * HDIM)):
            first = g * group_width + pair * 2 * HDIM
            head = first // HDIM
            values = scaled_ref[:, first : first + 2 * HDIM].astype(BF16)
            left = mm((affinity * head_decay(down, across, head, mask)).astype(BF16), values)
            right = mm((affinity * head_decay(down, across, head + 1, mask)).astype(BF16), values)
            pieces.append(jnp.where(lane < HDIM, left, right))
        y = jnp.concatenate(pieces, axis=1) + off
        y_ref[:, lanes] = y
        z = z_ref[:, lanes].astype(F32)
        gated = y * (z * jax.nn.sigmoid(z))
        normed = gated * group_inverse(gated, 0, group_width) * scale_ref[:, lanes]
        norm_own[lanes] = normed.T.astype(BF16)

    for d in order:
        span = at.span(d)
        value = pair_sum(span, 0)
        for j in range(1, at.outer):
            landed(far_in.at[j - 1, span], far_recv.at[j - 1, span])
            value = value + far_in[j - 1, span].astype(F32)
        if d == 0:
            ret_in[me] = value.astype(BF16)
        else:
            ret_out[span] = value.astype(BF16)
            push(ret_out.at[span], ret_in.at[me], ret_send.at[d], ret_recv.at[me], (span, t))
    w_there += w_ring.advance()
    value = own_grad_ref[...].astype(F32)
    value = value + mm(pick_ref[me], ret_in[me])
    for d in range(1, n_sp):
        span = at.span_back(d)
        landed(ret_in.at[span], ret_recv.at[span])
        value = value + mm(pick_ref[span], ret_in[span])
    mix_own[...] = value.astype(BF16)
    mix[:, cols(t)] = value.astype(BF16)
    for i, peer in enumerate(near):
        push(mix_own, mix.at[:, cols(t)], mix_send.at[0, i], mix_recv.at[t], (me, peer))
    for j, owner in enumerate(at.outers()):
        block = mix.at[:, cols(owner)]
        landed(block, mix_recv.at[owner])
        for i, partner in enumerate(at.partners()):
            push(block, block, mix_send.at[1 + j, i], mix_recv.at[owner], (me, partner))
    for partner in at.partners():
        core = lax.rem(partner, at.inner)
        for far in range(at.outer):
            owner = far * at.inner + core
            landed(mix.at[:, cols(owner)], mix_recv.at[owner])
    part_width = model_width // n_sp
    for k in range(n_sp):
        mix_parts[k] = mix[:, k * part_width : (k + 1) * part_width]

    total_ref[...] = jnp.zeros(total_ref.shape, F32)
    while True:
        for slot in w_there:
            total_ref[...] += mm(mix_parts[w_ring.origin(slot)], w_ring.block(slot)[...], 1, 1)
        if not w_ring.more():
            break
        w_there = w_ring.advance()
    norm_ring.advance()
    for g in range(groups):
        lanes = slice(g * group_width, (g + 1) * group_width)
        y, z = y_ref[:, lanes], z_ref[:, lanes].astype(F32)
        gate = jax.nn.sigmoid(z)
        silu = z * gate
        gated = y * silu
        inverse = group_inverse(gated, 0, group_width)
        unit = gated * inverse
        grad = total_ref[:, lanes] * scale_ref[:, lanes]
        grad = inverse * (grad - unit * jnp.mean(grad * unit, axis=1, keepdims=True))
        dgate_ref[:, lanes] = (grad * y * gate * (1.0 + z * (1.0 - gate))).astype(BF16)
        scan_grad = grad * silu
        g_ref[:, lanes] = scan_grad
        weighted = (scan_grad * grown_ref[:, lanes]).astype(BF16)
        reached = mm(weighted, c_ref[:, g * STATE : (g + 1) * STATE], 0, 0).astype(BF16)
        share = n_sp // groups
        reached_ref[g * share : (g + 1) * share] = reached.reshape(share, per, STATE)
    for d in range(1, n_sp):
        peer = at.span(d)
        push(reached_ref.at[peer], reached_in.at[me], reach_send.at[d], reach_recv.at[me], (peer, t))
    reached_in[me] = reached_ref[me]

    head_lane = lax.broadcasted_iota(jnp.int32, (tokens, heads), 1)
    head_down = lax.broadcasted_iota(jnp.int32, (heads, tokens), 0)
    sums = jnp.zeros((tokens, heads), F32)
    column_sums = jnp.zeros((heads, tokens), F32)
    for g in range(groups):
        states = slice(g * STATE, (g + 1) * STATE)
        lanes = slice(g * group_width, (g + 1) * group_width)
        b_rows, c_rows = b_ref[:, states], c_ref[:, states]
        affinity = mm(c_rows, b_rows, 1, 1)
        before = before_rows[lanes]
        affinity_grad = jnp.zeros((tokens, tokens), F32)
        for pair in range(group_width // (2 * HDIM)):
            first = g * group_width + pair * 2 * HDIM
            block = slice(first, first + 2 * HDIM)
            values = scaled_ref[:, block].astype(BF16)
            grads = g_ref[:, block].astype(BF16)
            halves = []
            for side in range(2):
                head = first // HDIM + side
                decay = head_decay(down, across, head, mask)
                own = grads * jnp.where((lane < HDIM) == (side == 0), 1.0, 0.0).astype(BF16)
                inner = mm(own, values, 1, 1) * decay
                affinity_grad = affinity_grad + inner
                moved = inner * affinity
                by_row = jnp.sum(moved, axis=1, keepdims=True)
                by_column = jnp.sum(moved, axis=0, keepdims=True)
                sums = sums + jnp.where(head_lane == head, by_row, 0.0)
                column_sums = column_sums + jnp.where(head_down == head, by_column, 0.0)
                halves.append(mm((affinity * decay).astype(BF16), grads, 0, 0))
            sgrad_ref[:, block] = jnp.where(lane < HDIM, halves[0], halves[1])
        grad = g_ref[:, lanes]
        grown = grown_ref[:, lanes]
        total_ref[:, lanes] = grad * (mm(c_rows, before, 1, 1) * grown)
        low = affinity_grad.astype(BF16)
        dc_ref[:, states] = (mm(low, b_rows) + mm((grad * grown).astype(BF16), before)).astype(BF16)
        dbp_ref[:, states] = mm(low, c_rows, 0, 0)
    through = mm(total_ref[...], wide, 1, 1, precision=HIGHEST)
    moved_ref[...] = sums - column_sums.T + through

    for d in range(1, n_sp):
        src_span = at.span_back(d)
        landed(reached_in.at[src_span], reach_recv.at[src_span])
    running = jnp.zeros(reached_ref.shape[1:], F32)
    for k in reversed(range(n_sp)):
        after_tmp[k] = running.astype(BF16)
        column = decay_column(lines_in[k], per)
        running = column * running + reached_in[k].astype(F32)
    for d in range(1, n_sp):
        peer = at.span(d)
        push(after_tmp.at[peer], later_in.at[me], later_send.at[d], later_recv.at[me], (peer, t))
    later_in[me] = after_tmp[me]
    share = tokens // n_tp

    def stripe(owner):
        return pl.ds(pl.multiple_of(owner * share, share), share)

    for d in range(1, n_sp):
        peer = at.span(d)
        push(
            mix_parts.at[peer, stripe(t)],
            mix_cols.at[me, stripe(t)],
            cols_send.at[d],
            cols_recv.at[me, t],
            (peer, t),
        )
    mix_cols[me] = mix_parts[me]
    norm_there = [0] + norm_ring.advance()
    for i in range(model_width // deep):
        piece = slice(i * deep, (i + 1) * deep)
        rows_t[piece] = rows[:, :, piece].reshape(pairs, deep).astype(F32).T.astype(BF16)
    hidden_t[...] = hidden_ref[...].astype(F32).T.astype(BF16)
    save(rows_t, rows_t_hbm)
    save(hidden_t, hidden_t_hbm)
    for d in range(1, n_sp):
        src_span = at.span_back(d)
        landed(later_in.at[src_span], later_recv.at[src_span])
    later_rows = later_in[...].reshape(n_sp * per, STATE)
    carried = []
    for g in range(groups):
        states = slice(g * STATE, (g + 1) * STATE)
        lanes = slice(g * group_width, (g + 1) * group_width)
        b_rows, later = b_ref[:, states], later_rows[lanes]
        ends, scaled = ends_ref[:, lanes], scaled_ref[:, lanes]
        from_later = mm(b_rows, later, 1, 1) * ends
        scaled_grad = sgrad_ref[:, lanes] + from_later
        total_ref[:, lanes] = scaled * from_later
        g_ref[:, lanes] = scaled_grad * x_ref[:, lanes].astype(F32)
        dx_ref[:, lanes] = (scaled_grad * step_wide[:, lanes]).astype(BF16)
        db_ref[:, states] = (dbp_ref[:, states] + mm((scaled * ends).astype(BF16), later)).astype(
            BF16
        )
        both = before_rows[lanes].astype(F32) * later.astype(F32)
        carried.append(jnp.sum(both, axis=1, keepdims=True))
    ended = mm(total_ref[...], wide, 1, 1, precision=HIGHEST)
    stepped = mm(g_ref[...], wide, 1, 1, precision=HIGHEST)
    both = jnp.broadcast_to(jnp.concatenate(carried, axis=0), (channels, STATE))
    carried = mm(jnp.ones((8, STATE), F32), mm(wide, both, precision=HIGHEST), 1, 1, HIGHEST)
    carried = carried[:1] * (1.0 / STATE) * jnp.exp(down[tokens - 1 : tokens, :])
    moved = moved_ref[...] - ended
    final = jnp.sum(ended, axis=0, keepdims=True) + carried
    lower = jnp.where(mask, 1.0, 0.0).astype(F32)
    decay_grad = mm(lower, moved, 0, 0, precision=HIGHEST) + final
    dstep_ref[...] = (stepped - rate_ref[...] * decay_grad).T

    for d in range(1, n_sp):
        src_span = at.span_back(d)
        block = mix_cols.at[src_span, stripe(t)]
        landed(block, cols_recv.at[src_span, t])
        for i, peer in enumerate(near):
            push(block, block, near_send.at[d, i], cols_recv.at[src_span, t], (me, peer))
    norm_there += norm_ring.advance()
    for d in range(1, n_sp):
        src_span = at.span_back(d)
        for j, owner in enumerate(at.outers()):
            block = mix_cols.at[src_span, stripe(owner)]
            landed(block, cols_recv.at[src_span, owner])
            for i, partner in enumerate(at.partners()):
                push(block, block, fwd_send.at[d, j, i], cols_recv.at[src_span, owner], (me, partner))
    for d in range(1, n_sp):
        src_span = at.span_back(d)
        for partner in at.partners():
            core = lax.rem(partner, at.inner)
            for far in range(at.outer):
                owner = far * at.inner + core
                landed(mix_cols.at[src_span, stripe(owner)], cols_recv.at[src_span, owner])
    proj_ref[...] = jnp.zeros(proj_ref.shape, F32)
    while True:
        for slot in norm_there:
            proj_ref[...] += mm(norm_ring.block(slot)[...], mix_cols[norm_ring.origin(slot)])
        if not norm_ring.more():
            break
        norm_there = norm_ring.advance()
    for wait in waits:
        wait()
    for copy in saves:
        copy.wait()


def main_part(stream, own_grad, routes, combine, weights, entering, scan_args, out_weight, n_sp, n_tp):
    tokens, width = own_grad.shape
    model_width, units = weights[0].shape
    capacity = -(-3 * tokens // n_sp)
    capacity = -(-capacity // 16) * 16
    pairs = n_sp * capacity
    x, step, rate, extra, b_rows, c_rows, gate, scale = scan_args
    channels = x.shape[1]
    heads = step.shape[0]
    per, lanes = channels // n_sp, entering.shape[1]
    out_columns = out_weight.shape[1]
    inner = 2 if n_tp % 2 == 0 else 1
    outer = n_tp // inner
    mates, others = max(inner - 1, 1), max(outer - 1, 1)
    near = max(inner + outer - 2, 1)
    blocks = (n_sp, capacity, width)
    states = (n_sp, per, lanes)

    def low(*shape):
        return pltpu.VMEM(shape, BF16)

    def full(*shape):
        return pltpu.VMEM(shape, F32)

    def out(shape, dtype):
        return jax.ShapeDtypeStruct(shape, dtype)

    anywhere = pl.BlockSpec(memory_space=pl.ANY)
    args = (stream, own_grad, routes, combine, *weights, entering, *scan_args, out_weight)
    return pl.pallas_call(
        functools.partial(main_kernel, n_sp, n_tp),
        out_shape=(
            out((model_width, pairs), BF16),
            out((n_sp, capacity, model_width), BF16),
            out((units, pairs), BF16),
            out((pairs, units), BF16),
            out((pairs, units), BF16),
            out((channels, out_columns), F32),
            out(x.shape, BF16),
            out(step.shape, F32),
            out(b_rows.shape, BF16),
            out(c_rows.shape, BF16),
            out(x.shape, BF16),
        ),
        in_specs=whole(4) + [anywhere] * 3 + whole(len(args) - 7),
        out_specs=tuple([anywhere] * 5 + whole(6)),
        scratch_shapes=[
            low(n_sp, capacity, model_width),
            low(n_sp, capacity, model_width),
            low(model_width, pairs),
            low(pairs, units),
            low(units, pairs),
            low(pairs, units),
            low(pairs, units),
            low(*blocks),
            low(*blocks),
            low(n_sp, tokens, capacity),
            low(*states),
            low(*states),
            low(n_sp, 1, lanes),
            low(n_sp, 1, lanes),
            DMA((2, n_sp)),
            DMA((2, n_sp, near)),
            DMA((2, n_sp, max((outer - 1) * (inner - 1), 1))),
            DMA((2, n_sp, n_tp)),
            DMA((n_sp,)),
            DMA((n_sp,)),
            DMA((n_sp,)),
            DMA((n_sp,)),
            DMA((5,)),
            low(model_width, units),
            low(model_width, units),
            low(units, model_width),
            full(pairs, units),
            full(pairs, units),
            full(pairs, units),
            low(n_sp, capacity, model_width),
            low(mates, outer, *blocks),
            low(others, *blocks),
            low(others, *blocks),
            low(*blocks),
            low(*blocks),
            low(*states),
            low(*states),
            low(tokens, width),
            low(tokens, model_width),
            low(n_sp, tokens, out_columns),
            low(n_sp, tokens, out_columns),
            low(n_sp, channels, out_columns),
            low(channels, tokens),
            low(n_sp, channels, tokens),
            full(tokens, channels),
            full(tokens, channels),
            full(tokens, channels),
            full(tokens, channels),
            full(tokens, channels),
            full(tokens, channels),
            full(tokens, channels),
            full(*b_rows.shape),
            full(tokens, heads),
            low(*states),
            low(*states),
            low(*states),
            low(*states),
            DMA((3,)),
            DMA((mates, outer, n_sp)),
            DMA((mates, outer, n_sp)),
            DMA((others, n_sp)),
            DMA((others, n_sp)),
            DMA((n_sp,)),
            DMA((n_sp,)),
            DMA((outer, near)),
            DMA((n_tp,)),
            DMA((n_sp,)),
            DMA((n_sp,)),
            DMA((n_sp, 2)),
            DMA((n_sp, 2)),
            DMA((n_sp, 2)),
            DMA((n_sp, 2)),
            DMA((n_sp,)),
            DMA((n_sp,)),
            DMA((n_sp,)),
            DMA((n_sp,)),
            DMA((n_sp,)),
            DMA((n_sp, near)),
            DMA((n_sp, others, mates)),
            DMA((n_sp, n_tp)),
        ],
        compiler_params=pltpu.CompilerParams(
            collective_id=2, has_side_effects=True, vmem_limit_bytes=67_000_000
        ),
        name="main_part",
    )(*args)


def weight_grad_kernel(count, rows_ref, hidden_ref, sent_ref, gate_ref, up_ref, *rest):
    ready, (g_out, u_out, d_out), out = rest[:count], rest[count : count + 3], rest[count + 3 :]
    capacity = sent_ref.shape[1]
    sent = sent_ref[...].reshape(sent_ref.shape[0] * capacity, sent_ref.shape[2])
    g_out[...] = mm(rows_ref[...], gate_ref[...]).astype(BF16)
    u_out[...] = mm(rows_ref[...], up_ref[...]).astype(BF16)
    d_out[...] = mm(hidden_ref[...], sent).astype(BF16)
    for source, target in zip(ready, out):
        target[...] = source[...]


def expert_weight_grads(rows_t, sent, hidden_t, gate_grad, up_grad, ready):
    model_width, pairs = rows_t.shape
    units = hidden_t.shape[0]
    tile = 512
    steps = model_width // tile
    fixed = pl.BlockSpec((pairs, units), lambda i: (0, 0))
    tall = pl.BlockSpec((tile, units), lambda i: (i, 0))
    handed = []
    for array in ready:
        if array.shape[0] % (16 * steps):
            handed.append(pl.BlockSpec(array.shape, lambda i: (0, 0)))
        else:
            handed.append(pl.BlockSpec((array.shape[0] // steps, array.shape[1]), lambda i: (i, 0)))
    return pl.pallas_call(
        functools.partial(weight_grad_kernel, len(ready)),
        grid=(steps,),
        out_shape=(
            jax.ShapeDtypeStruct((model_width, units), BF16),
            jax.ShapeDtypeStruct((model_width, units), BF16),
            jax.ShapeDtypeStruct((units, model_width), BF16),
            *(jax.ShapeDtypeStruct(array.shape, array.dtype) for array in ready),
        ),
        in_specs=[
            pl.BlockSpec((tile, pairs), lambda i: (i, 0)),
            pl.BlockSpec((units, pairs), lambda i: (0, 0)),
            pl.BlockSpec(sent.shape[:2] + (tile,), lambda i: (0, 0, i)),
            fixed,
            fixed,
            *handed,
        ],
        out_specs=(tall, tall, pl.BlockSpec((units, tile), lambda i: (0, i)), *handed),
        name="expert_weight_grads",
    )(rows_t, hidden_t, sent, gate_grad, up_grad, *ready)


def body(
    mixer_output_stream,
    layer_output_gradient,
    routes,
    expert_combine_weight,
    expert_gate_weight,
    expert_up_weight,
    expert_down_weight,
    head_mixer_input,
    head_step_size,
    head_decay_rate,
    extra_log_decay,
    state_entering_span,
    state_input_vectors,
    state_readout_vectors,
    gate_preactivation,
    group_norm_scale,
    mixer_output_weight,
):
    n_sp, n_tp = lax.axis_size("sp"), lax.axis_size("tp")
    rows_t, sent, hidden_t, gate_grad, up_grad, *ready = main_part(
        mixer_output_stream,
        layer_output_gradient,
        routes.T,
        expert_combine_weight.T,
        (expert_gate_weight[0], expert_up_weight[0], expert_down_weight[0]),
        state_entering_span.reshape(-1, STATE),
        (
            head_mixer_input,
            head_step_size.T,
            head_decay_rate[None, :],
            extra_log_decay.T,
            state_input_vectors,
            state_readout_vectors,
            gate_preactivation,
            group_norm_scale[None, :],
        ),
        mixer_output_weight,
        n_sp,
        n_tp,
    )
    grad_g, grad_u, grad_d, proj_grad, input_grad, step_grad, b_grad, c_grad, gate_grad_in = (
        expert_weight_grads(rows_t, sent, hidden_t, gate_grad, up_grad, ready)
    )
    return (
        grad_g[None],
        grad_u[None],
        grad_d[None],
        proj_grad,
        input_grad,
        step_grad.T,
        b_grad,
        c_grad,
        gate_grad_in,
    )


def solution(mesh):
    return jax.shard_map(
        body,
        mesh=mesh,
        in_specs=(
            P("sp", "tp"),
            P("sp", "tp"),
            P("sp", None),
            P("sp", None),
            P("sp", None, "tp"),
            P("sp", None, "tp"),
            P("sp", "tp", None),
            P("sp", "tp"),
            P("sp", "tp"),
            P("tp"),
            P("sp", "tp"),
            P("tp", None, None),
            P("sp", "tp"),
            P("sp", "tp"),
            P("sp", "tp"),
            P("tp"),
            P("tp", "sp"),
        ),
        out_specs=(
            P("sp", None, "tp"),
            P("sp", None, "tp"),
            P("sp", "tp", None),
            P("tp", "sp"),
            P("sp", "tp"),
            P("sp", "tp"),
            P("sp", "tp"),
            P("sp", "tp"),
            P("sp", "tp"),
        ),
        check_vma=False,
    )
```

```python
import functools

import jax
import jax.numpy as jnp
from jax import lax
from jax.experimental import pallas as pl
from jax.experimental.pallas import tpu as pltpu
from jax.sharding import PartitionSpec as P

HDIM = 64
STATE = 128
BLK = 128


norm_eps = 1e-05
exact_mode = lax.Precision.HIGH


MESH = pl.DeviceIdType.MESH
BF16 = jnp.bfloat16
F32 = jnp.float32
DMA = pltpu.SemaphoreType.DMA


class Place:
    def __init__(self, n_sp, n_tp):
        self.n_sp, self.n_tp = n_sp, n_tp
        self.inner = 2 if n_tp % 2 == 0 else 1
        self.outer = n_tp // self.inner
        self.me = lax.axis_index("sp")
        self.t = lax.axis_index("tp")
        self.core = lax.rem(self.t, self.inner)
        self.far = lax.div(self.t, self.inner)

    def span(self, d):
        return lax.rem(self.me + d, self.n_sp)

    def span_back(self, d):
        return lax.rem(self.me + (self.n_sp - d), self.n_sp)

    def partners(self):
        return [self.far * self.inner + lax.rem(self.core + i, self.inner) for i in range(1, self.inner)]

    def outers(self):
        return [lax.rem(self.far + j, self.outer) * self.inner + self.core for j in range(1, self.outer)]

    def enter(self, with_span=True):
        barrier = pltpu.get_barrier_semaphore()
        devices = [(self.me, p) for p in self.partners() + self.outers()]
        if with_span:
            devices += [(self.span(d), self.t) for d in range(1, self.n_sp)]
        for device in devices:
            pl.semaphore_signal(barrier, inc=1, device_id=device, device_id_type=MESH)
        pl.semaphore_wait(barrier, len(devices))


def remote(src, dst, send, recv, device):
    return pltpu.make_async_remote_copy(
        src_ref=src, dst_ref=dst, send_sem=send, recv_sem=recv, device_id=device, device_id_type=MESH
    )


def decay_column(row, per):
    width = row.shape[-1]
    down = lax.broadcasted_iota(jnp.int32, (per, width), 0)
    across = lax.broadcasted_iota(jnp.int32, (per, width), 1)
    spread = jnp.broadcast_to(row.astype(F32), (per, width))
    return jnp.sum(jnp.where(down == across, spread, 0.0), axis=1, keepdims=True)


def whole(count):
    return [pl.BlockSpec(memory_space=pltpu.VMEM)] * count


HIGHEST = lax.Precision.HIGHEST


def mm(x, y, xd=1, yd=0, precision=None):
    return lax.dot_general(
        x, y, (((xd,), (yd,)), ((), ())), precision=precision, preferred_element_type=F32
    )


def lower_ones(size):
    down = lax.broadcasted_iota(jnp.int32, (size, size), 0)
    across = lax.broadcasted_iota(jnp.int32, (size, size), 1)
    return down >= across


def head_ones(heads, channels):
    down = lax.broadcasted_iota(jnp.int32, (heads, channels), 0)
    across = lax.broadcasted_iota(jnp.int32, (heads, channels), 1)
    return jnp.where(lax.div(across, HDIM) == down, 1.0, 0.0).astype(F32)


def turned(x):
    size = x.shape[1]
    down = lax.broadcasted_iota(jnp.int32, (size, size), 0)
    across = lax.broadcasted_iota(jnp.int32, (size, size), 1)
    return mm(jnp.where(down == across, 1.0, 0.0).astype(F32), x, 1, 1, HIGHEST)


def log_decay_sums(step_ref, rate_ref, extra_ref):
    heads, tokens = step_ref.shape
    log_decay = extra_ref[...] - step_ref[...] * decay_column(rate_ref[...], heads)
    lower = jnp.where(lower_ones(tokens), 1.0, 0.0).astype(F32)
    down = mm(lower, log_decay, 1, 1, HIGHEST)
    across = mm(log_decay, lower, 1, 1, HIGHEST)
    return down, across


def head_decay(down, across, head, mask):
    gap = down[:, head : head + 1] - across[head : head + 1, :]
    return jnp.where(mask, jnp.exp(jnp.where(mask, gap, 0.0)), 0.0)


def group_inverse(gated, group, width):
    part = gated[:, group * width : (group + 1) * width]
    return lax.rsqrt(jnp.mean(part * part, axis=1, keepdims=True) + norm_eps)


def ring_origin(position, count):
    position = lax.rem(position + 2 * count, count)
    return jnp.where(2 * position < count, 2 * position, 2 * count - 1 - 2 * position)


def ring_position(me, count):
    half = lax.div(me, 2)
    return jnp.where(lax.rem(me, 2) == 0, half, count - 1 - half)


class Circle:
    def __init__(self, at, own, slots, sends, recvs, waits):
        self.at, self.own, self.slots = at, own, slots
        self.sends, self.recvs, self.waits = sends, recvs, waits
        self.half = at.n_sp // 2
        self.position = ring_position(at.me, at.n_sp)
        self.after = ring_origin(self.position + 1, at.n_sp)
        self.prior = ring_origin(self.position - 1, at.n_sp)
        self.step = 0

    def block(self, slot):
        return self.own if slot == 0 else self.slots.at[slot]

    def origin(self, slot):
        shift = -slot if slot <= self.half else slot - self.half
        return ring_origin(self.position + shift, self.at.n_sp)

    def part(self, block, p):
        size = self.own.shape[0] // 2
        return block.at[pl.ds(p * size, size)]

    def send(self, source, slot, p, peer):
        copy = remote(
            self.part(source, p),
            self.part(self.slots.at[slot], p),
            self.sends.at[slot, p],
            self.recvs.at[slot, p],
            (peer, self.at.t),
        )
        copy.start()
        self.waits.append(copy.wait_send)

    def landed(self, slot, p):
        block = self.part(self.slots.at[slot], p)
        pltpu.make_async_copy(block, block, self.recvs.at[slot, p]).wait()

    def advance(self):
        half, step = self.half, self.step
        self.step = step + 1
        front, rear = self.block(step), self.block(half + step if step else 0)
        for p in range(2):
            if step and step <= half:
                self.landed(step, p)
            if step and step < half:
                self.landed(half + step, p)
            if step + 1 < half:
                self.send(front, step + 1, p, self.after)
                self.send(rear, half + step + 1, p, self.prior)
            elif step + 1 == half and p == 0:
                self.send(front, half, p, self.after)
            elif step + 1 == half:
                self.send(rear, half, p, self.prior)
        if step == 0:
            return [0]
        return [step, half + step] if step < half else [step]

    def more(self):
        return self.step <= self.half


def main_kernel(
    n_sp,
    n_tp,
    stream_ref,
    own_grad_ref,
    routes_ref,
    combine_ref,
    wg_hbm,
    wu_hbm,
    wd_hbm,
    entering_ref,
    x_ref,
    step_ref,
    rate_ref,
    extra_ref,
    b_ref,
    c_ref,
    z_ref,
    scale_ref,
    out_w_ref,
    rows_t_hbm,
    down_hbm,
    gate_grad_hbm,
    up_grad_hbm,
    proj_hbm,
    dx_hbm,
    dstep_hbm,
    db_hbm,
    dc_hbm,
    dgate_hbm,
    proj_ref,
    dx_ref,
    dstep_ref,
    db_ref,
    dc_ref,
    dgate_ref,
    rows,
    sent,
    rows_t,
    hidden_ref,
    hidden_t,
    gate_grad_ref,
    up_grad_ref,
    rows_out,
    sent_out,
    pick_ref,
    state_out,
    state_in,
    lines_out,
    lines_in,
    span_send,
    tp_send,
    tp_fwd_send,
    block_recv,
    state_send,
    state_recv,
    lines_send,
    lines_recv,
    save_sem,
    wg,
    wu,
    wd,
    acc_gate,
    acc_up,
    acc_down,
    part,
    pair_in,
    far_out,
    far_in,
    ret_out,
    ret_in,
    before_tmp,
    before_in,
    mix_own,
    mix,
    mix_parts,
    mix_cols,
    w_slots,
    norm_own,
    norm_slots,
    y_ref,
    total_ref,
    scaled_ref,
    grown_ref,
    ends_ref,
    g_ref,
    sgrad_ref,
    dbp_ref,
    moved_ref,
    reached_ref,
    reached_in,
    after_tmp,
    later_in,
    load_sem,
    pair_send,
    pair_recv,
    far_send,
    far_recv,
    ret_send,
    ret_recv,
    mix_send,
    mix_recv,
    back_send,
    back_recv,
    w_send,
    w_recv,
    norm_send,
    norm_recv,
    reach_send,
    reach_recv,
    later_send,
    later_recv,
    cols_send,
    near_send,
    fwd_send,
    cols_recv,
):
    at = Place(n_sp, n_tp)
    me, t = at.me, at.t
    width = own_grad_ref.shape[1]
    _, capacity, model_width = rows.shape
    pairs = n_sp * capacity
    tokens, channels = x_ref.shape
    per = channels // n_sp
    heads = step_ref.shape[0]
    groups = b_ref.shape[1] // STATE
    group_width = channels // groups
    waits = []

    def cols(owner):
        return pl.ds(pl.multiple_of(owner * width, width), width)

    def landed(block, sem):
        pltpu.make_async_copy(block, block, sem).wait()

    def push(source, target, send, recv, device):
        copy = remote(source, target, send, recv, device)
        copy.start()
        waits.append(copy.wait_send)

    loads = []
    for i, (source, target) in enumerate(((wg_hbm, wg), (wu_hbm, wu), (wd_hbm, wd))):
        loads.append(pltpu.make_async_copy(source, target, load_sem.at[i]))
        loads[-1].start()
    at.enter()
    w_ring = Circle(at, out_w_ref, w_slots, w_send, w_recv, waits)
    norm_ring = Circle(at, norm_own, norm_slots, norm_send, norm_recv, waits)
    w_ring.advance()

    routes = turned(routes_ref[...].astype(F32))
    combine = turned(combine_ref[...])
    top = routes.shape[1]
    expert_lane = lax.broadcasted_iota(jnp.int32, (tokens, n_sp), 1).astype(F32)
    slot_lane = lax.broadcasted_iota(jnp.int32, (tokens, capacity), 1).astype(F32)
    mask = lower_ones(tokens)
    named = [routes[:, k : k + 1] == expert_lane for k in range(top)]
    ones = sum(jnp.where(n, 1.0, 0.0) for n in named)
    earlier = mm(jnp.where(mask, 1.0, 0.0).astype(BF16), ones.astype(BF16)) - ones
    weighted = [
        (own_grad_ref[...].astype(F32) * combine[:, k : k + 1]).astype(BF16) for k in range(top)
    ]
    places = [jnp.sum(jnp.where(n, earlier, 0.0), axis=1, keepdims=True) for n in named]
    for e in range(n_sp):
        picks = []
        for k in range(top):
            place = jnp.where(routes[:, k : k + 1] == float(e), places[k], -1.0)
            picks.append(jnp.where(place == slot_lane, 1.0, 0.0).astype(BF16))
        pick = sum(picks)
        pick_ref[e] = pick
        rows_out[e] = mm(pick, stream_ref[...], 0, 0).astype(BF16)
        sent_out[e] = sum(mm(p, w, 0, 0) for p, w in zip(picks, weighted)).astype(BF16)
    both = ((rows_out, rows), (sent_out, sent))
    for d in range(1, n_sp):
        peer = at.span(d)
        for a, (source, target) in enumerate(both):
            push(
                source.at[peer],
                target.at[me, :, cols(t)],
                span_send.at[a, d],
                block_recv.at[a, me, t],
                (peer, t),
            )

    def pass_on(d, sources, peers, owner, sems, base):
        src_span = at.span_back(d)
        for a in range(2):
            for i, peer in enumerate(peers):
                push(
                    sources[a],
                    both[a][1].at[src_span, :, cols(owner)],
                    sems.at[a, d, base + i],
                    block_recv.at[a, src_span, owner],
                    (me, peer),
                )

    def block_landed(a, src_span, owner):
        landed(both[a][1].at[src_span, :, cols(owner)], block_recv.at[a, src_span, owner])

    near = at.outers() + at.partners()
    pass_on(0, [rows_out.at[me], sent_out.at[me]], near, t, tp_send, 0)
    rows[me, :, cols(t)] = rows_out[me]
    sent[me, :, cols(t)] = sent_out[me]

    down, across = log_decay_sums(step_ref, rate_ref, extra_ref)
    wide = head_ones(heads, channels)
    lane = lax.broadcasted_iota(jnp.int32, (tokens, 2 * HDIM), 1)
    step_wide = mm(turned(step_ref[...]), wide, precision=HIGHEST)
    scaled_ref[...] = x_ref[...].astype(F32) * step_wide
    down_wide = mm(down, wide, precision=HIGHEST)
    grown_ref[...] = jnp.exp(down_wide)
    ends_ref[...] = jnp.exp(down_wide[tokens - 1 : tokens, :] - down_wide)
    spans = n_sp // groups
    for g in range(groups):
        lanes = slice(g * group_width, (g + 1) * group_width)
        left = (scaled_ref[:, lanes] * ends_ref[:, lanes]).astype(BF16)
        state = mm(left, b_ref[:, g * STATE : (g + 1) * STATE], 0, 0).astype(BF16)
        state_out[g * spans : (g + 1) * spans] = state.reshape(spans, per, STATE)
    whole_decay = jnp.exp(down_wide[tokens - 1 : tokens, :])
    lines_out[...] = jnp.zeros(lines_out.shape, BF16)
    for k in range(n_sp):
        lines_out[k, :, :per] = whole_decay[:, k * per : (k + 1) * per].astype(BF16)
    for d in range(1, n_sp):
        peer = at.span(d)
        push(state_out.at[peer], state_in.at[me], state_send.at[d], state_recv.at[me], (peer, t))
        push(lines_out.at[peer], lines_in.at[me], lines_send.at[d], lines_recv.at[me], (peer, t))
    state_in[me] = state_out[me]
    lines_in[me] = lines_out[me]

    for d in range(1, n_sp):
        src_span = at.span_back(d)
        for a in range(2):
            block_landed(a, src_span, t)
        pass_on(d, [b[1].at[src_span, :, cols(t)] for b in both], near, t, tp_send, 0)
    for d in range(n_sp):
        src_span = at.span_back(d)
        for j, owner in enumerate(at.outers()):
            for a in range(2):
                block_landed(a, src_span, owner)
            pass_on(
                d,
                [b[1].at[src_span, :, cols(owner)] for b in both],
                at.partners(),
                owner,
                tp_fwd_send,
                j * (at.inner - 1),
            )
    for d in range(1, n_sp):
        src_span = at.span_back(d)
        landed(state_in.at[src_span], state_recv.at[src_span])
        landed(lines_in.at[src_span], lines_recv.at[src_span])
    running = entering_ref[pl.ds(pl.multiple_of(me * per, per), per), :]
    for k in range(n_sp):
        before_tmp[k] = running.astype(BF16)
        running = decay_column(lines_in[k], per) * running + state_in[k].astype(F32)
    for d in range(1, n_sp):
        peer = at.span(d)
        push(before_tmp.at[peer], before_in.at[me], back_send.at[d], back_recv.at[me], (peer, t))
    before_in[me] = before_tmp[me]
    w_there = [0] + w_ring.advance()
    for d in range(n_sp):
        src_span = at.span_back(d)
        for partner in at.partners():
            core = lax.rem(partner, at.inner)
            for far in range(at.outer):
                for a in range(2):
                    block_landed(a, src_span, far * at.inner + core)

    saves = []

    def save(source, target):
        copy = pltpu.make_async_copy(source, target, save_sem.at[len(saves)])
        copy.start()
        saves.append(copy)

    deep = 256

    def chunk(i):
        return pl.ds(pl.multiple_of(i * deep, deep), deep)

    acc_gate[...] = jnp.zeros(acc_gate.shape, F32)
    acc_up[...] = jnp.zeros(acc_up.shape, F32)
    acc_down[...] = jnp.zeros(acc_down.shape, F32)
    loads[0].wait()

    @pl.loop(0, model_width // deep)
    def _(i):
        acc_gate[...] += mm(rows[:, :, chunk(i)].reshape(pairs, deep), wg[chunk(i), :])

    loads[1].wait()

    @pl.loop(0, model_width // deep)
    def _(i):
        acc_up[...] += mm(rows[:, :, chunk(i)].reshape(pairs, deep), wu[chunk(i), :])

    loads[2].wait()

    @pl.loop(0, model_width // deep)
    def _(i):
        acc_down[...] += mm(sent[:, :, chunk(i)].reshape(pairs, deep), wd[:, chunk(i)], 1, 1)

    @pl.loop(0, n_sp)
    def _(i):
        piece = pl.ds(pl.multiple_of(i * capacity, capacity), capacity)
        pre_gate, pre_up, hidden_grad = acc_gate[piece, :], acc_up[piece, :], acc_down[piece, :]
        gate = jax.nn.sigmoid(pre_gate)
        silu = pre_gate * gate
        hidden_ref[piece, :] = (silu * pre_up).astype(BF16)
        slope = gate * (1.0 + pre_gate * (1.0 - gate))
        gate_grad_ref[piece, :] = (hidden_grad * pre_up * slope).astype(BF16)
        up_grad_ref[piece, :] = (hidden_grad * silu).astype(BF16)

    order = list(range(1, n_sp)) + [0]
    fars = list(range(1, at.outer)) + [0]

    def partial_columns(owner):
        rows = cols(owner)
        value = mm(gate_grad_ref[...], wg[rows, :], 1, 1) + mm(up_grad_ref[...], wu[rows, :], 1, 1)
        part[:, :, rows] = value.astype(BF16).reshape(n_sp, capacity, width)

    for i, partner in enumerate(at.partners()):
        core = lax.rem(partner, at.inner)
        for j in fars:
            far = lax.rem(at.far + j, at.outer)
            owner = far * at.inner + core
            partial_columns(owner)
            for d in order:
                span = at.span(d)
                push(
                    part.at[span, :, cols(owner)],
                    pair_in.at[i, j, span],
                    pair_send.at[i, j, d],
                    pair_recv.at[i, j, span],
                    (me, partner),
                )
    for j in fars:
        partial_columns(lax.rem(at.far + j, at.outer) * at.inner + at.core)

    def pair_sum(span, j):
        far = lax.rem(at.far + j, at.outer)
        value = part[span, :, cols(far * at.inner + at.core)].astype(F32)
        for i in range(at.inner - 1):
            value = value + pair_in[i, j, span].astype(F32)
        return value

    for d in order:
        span = at.span(d)
        for j in fars:
            for i in range(at.inner - 1):
                landed(pair_in.at[i, j, span], pair_recv.at[i, j, span])
            if j:
                far_out[j - 1, span] = pair_sum(span, j).astype(BF16)
                push(
                    far_out.at[j - 1, span],
                    far_in.at[j - 1, span],
                    far_send.at[j - 1, d],
                    far_recv.at[j - 1, span],
                    (me, lax.rem(at.far + j, at.outer) * at.inner + at.core),
                )
    w_there += w_ring.advance()
    save(gate_grad_ref, gate_grad_hbm)
    save(up_grad_ref, up_grad_hbm)

    for d in range(1, n_sp):
        src_span = at.span_back(d)
        landed(before_in.at[src_span], back_recv.at[src_span])
    before_rows = before_in[...].reshape(n_sp * per, STATE)
    for g in range(groups):
        states = slice(g * STATE, (g + 1) * STATE)
        lanes = slice(g * group_width, (g + 1) * group_width)
        b_rows, c_rows = b_ref[:, states], c_ref[:, states]
        affinity = mm(c_rows, b_rows, 1, 1)
        off = mm(c_rows, before_rows[lanes], 1, 1) * grown_ref[:, lanes]
        pieces = []
        for pair in range(group_width // (2 * HDIM)):
            first = g * group_width + pair * 2 * HDIM
            head = first // HDIM
            values = scaled_ref[:, first : first + 2 * HDIM].astype(BF16)
            left = mm((affinity * head_decay(down, across, head, mask)).astype(BF16), values)
            right = mm((affinity * head_decay(down, across, head + 1, mask)).astype(BF16), values)
            pieces.append(jnp.where(lane < HDIM, left, right))
        y = jnp.concatenate(pieces, axis=1) + off
        y_ref[:, lanes] = y
        z = z_ref[:, lanes].astype(F32)
        gated = y * (z * jax.nn.sigmoid(z))
        normed = gated * group_inverse(gated, 0, group_width) * scale_ref[:, lanes]
        norm_own[lanes] = normed.T.astype(BF16)

    for d in order:
        span = at.span(d)
        value = pair_sum(span, 0)
        for j in range(1, at.outer):
            landed(far_in.at[j - 1, span], far_recv.at[j - 1, span])
            value = value + far_in[j - 1, span].astype(F32)
        if d == 0:
            ret_in[me] = value.astype(BF16)
        else:
            ret_out[span] = value.astype(BF16)
            push(ret_out.at[span], ret_in.at[me], ret_send.at[d], ret_recv.at[me], (span, t))
    w_there += w_ring.advance()
    value = own_grad_ref[...].astype(F32)
    value = value + mm(pick_ref[me], ret_in[me])
    for d in range(1, n_sp):
        span = at.span_back(d)
        landed(ret_in.at[span], ret_recv.at[span])
        value = value + mm(pick_ref[span], ret_in[span])
    mix_own[...] = value.astype(BF16)
    mix[:, cols(t)] = value.astype(BF16)
    for i, peer in enumerate(near):
        push(mix_own, mix.at[:, cols(t)], mix_send.at[0, i], mix_recv.at[t], (me, peer))
    for j, owner in enumerate(at.outers()):
        block = mix.at[:, cols(owner)]
        landed(block, mix_recv.at[owner])
        for i, partner in enumerate(at.partners()):
            push(block, block, mix_send.at[1 + j, i], mix_recv.at[owner], (me, partner))
    for partner in at.partners():
        core = lax.rem(partner, at.inner)
        for far in range(at.outer):
            owner = far * at.inner + core
            landed(mix.at[:, cols(owner)], mix_recv.at[owner])
    part_width = model_width // n_sp
    for k in range(n_sp):
        mix_parts[k] = mix[:, k * part_width : (k + 1) * part_width]

    total_ref[...] = jnp.zeros(total_ref.shape, F32)
    while True:
        for slot in w_there:
            total_ref[...] += mm(mix_parts[w_ring.origin(slot)], w_ring.block(slot)[...], 1, 1)
        if not w_ring.more():
            break
        w_there = w_ring.advance()
    norm_ring.advance()
    for g in range(groups):
        lanes = slice(g * group_width, (g + 1) * group_width)
        y, z = y_ref[:, lanes], z_ref[:, lanes].astype(F32)
        gate = jax.nn.sigmoid(z)
        silu = z * gate
        gated = y * silu
        inverse = group_inverse(gated, 0, group_width)
        unit = gated * inverse
        grad = total_ref[:, lanes] * scale_ref[:, lanes]
        grad = inverse * (grad - unit * jnp.mean(grad * unit, axis=1, keepdims=True))
        dgate_ref[:, lanes] = (grad * y * gate * (1.0 + z * (1.0 - gate))).astype(BF16)
        scan_grad = grad * silu
        g_ref[:, lanes] = scan_grad
        weighted = (scan_grad * grown_ref[:, lanes]).astype(BF16)
        reached = mm(weighted, c_ref[:, g * STATE : (g + 1) * STATE], 0, 0).astype(BF16)
        share = n_sp // groups
        reached_ref[g * share : (g + 1) * share] = reached.reshape(share, per, STATE)
    for d in range(1, n_sp):
        peer = at.span(d)
        push(reached_ref.at[peer], reached_in.at[me], reach_send.at[d], reach_recv.at[me], (peer, t))
    reached_in[me] = reached_ref[me]

    head_lane = lax.broadcasted_iota(jnp.int32, (tokens, heads), 1)
    head_down = lax.broadcasted_iota(jnp.int32, (heads, tokens), 0)
    sums = jnp.zeros((tokens, heads), F32)
    column_sums = jnp.zeros((heads, tokens), F32)
    for g in range(groups):
        states = slice(g * STATE, (g + 1) * STATE)
        lanes = slice(g * group_width, (g + 1) * group_width)
        b_rows, c_rows = b_ref[:, states], c_ref[:, states]
        affinity = mm(c_rows, b_rows, 1, 1)
        before = before_rows[lanes]
        affinity_grad = jnp.zeros((tokens, tokens), F32)
        for pair in range(group_width // (2 * HDIM)):
            first = g * group_width + pair * 2 * HDIM
            block = slice(first, first + 2 * HDIM)
            values = scaled_ref[:, block].astype(BF16)
            grads = g_ref[:, block].astype(BF16)
            halves = []
            for side in range(2):
                head = first // HDIM + side
                decay = head_decay(down, across, head, mask)
                own = grads * jnp.where((lane < HDIM) == (side == 0), 1.0, 0.0).astype(BF16)
                inner = mm(own, values, 1, 1) * decay
                affinity_grad = affinity_grad + inner
                moved = inner * affinity
                by_row = jnp.sum(moved, axis=1, keepdims=True)
                by_column = jnp.sum(moved, axis=0, keepdims=True)
                sums = sums + jnp.where(head_lane == head, by_row, 0.0)
                column_sums = column_sums + jnp.where(head_down == head, by_column, 0.0)
                halves.append(mm((affinity * decay).astype(BF16), grads, 0, 0))
            sgrad_ref[:, block] = jnp.where(lane < HDIM, halves[0], halves[1])
        grad = g_ref[:, lanes]
        grown = grown_ref[:, lanes]
        total_ref[:, lanes] = grad * (mm(c_rows, before, 1, 1) * grown)
        low = affinity_grad.astype(BF16)
        dc_ref[:, states] = (mm(low, b_rows) + mm((grad * grown).astype(BF16), before)).astype(BF16)
        dbp_ref[:, states] = mm(low, c_rows, 0, 0)
    through = mm(total_ref[...], wide, 1, 1, precision=HIGHEST)
    moved_ref[...] = sums - column_sums.T + through

    save(dc_ref, dc_hbm)
    save(dgate_ref, dgate_hbm)
    norm_there = [0] + norm_ring.advance()

    for d in range(1, n_sp):
        src_span = at.span_back(d)
        landed(reached_in.at[src_span], reach_recv.at[src_span])
    running = jnp.zeros(reached_ref.shape[1:], F32)
    for k in reversed(range(n_sp)):
        after_tmp[k] = running.astype(BF16)
        column = decay_column(lines_in[k], per)
        running = column * running + reached_in[k].astype(F32)
    for d in range(1, n_sp):
        peer = at.span(d)
        push(after_tmp.at[peer], later_in.at[me], later_send.at[d], later_recv.at[me], (peer, t))
    later_in[me] = after_tmp[me]
    share = tokens // n_tp

    def stripe(owner):
        return pl.ds(pl.multiple_of(owner * share, share), share)

    for d in range(1, n_sp):
        peer = at.span(d)
        push(
            mix_parts.at[peer, stripe(t)],
            mix_cols.at[me, stripe(t)],
            cols_send.at[d],
            cols_recv.at[me, t],
            (peer, t),
        )
    mix_cols[me] = mix_parts[me]
    norm_there += norm_ring.advance()
    for i in range(model_width // deep):
        piece = slice(i * deep, (i + 1) * deep)
        rows_t[piece] = rows[:, :, piece].reshape(pairs, deep).astype(F32).T.astype(BF16)
    hidden_t[...] = hidden_ref[...].astype(F32).T.astype(BF16)
    save(rows_t, rows_t_hbm)
    for i in range(n_tp):
        piece = slice(i * width, (i + 1) * width)
        wd[:, piece] = mm(hidden_t[...], sent[:, :, piece].reshape(pairs, width)).astype(BF16)
    save(wd, down_hbm)
    for d in range(1, n_sp):
        src_span = at.span_back(d)
        landed(later_in.at[src_span], later_recv.at[src_span])
    later_rows = later_in[...].reshape(n_sp * per, STATE)
    carried = []
    for g in range(groups):
        states = slice(g * STATE, (g + 1) * STATE)
        lanes = slice(g * group_width, (g + 1) * group_width)
        b_rows, later = b_ref[:, states], later_rows[lanes]
        ends, scaled = ends_ref[:, lanes], scaled_ref[:, lanes]
        from_later = mm(b_rows, later, 1, 1) * ends
        scaled_grad = sgrad_ref[:, lanes] + from_later
        total_ref[:, lanes] = scaled * from_later
        g_ref[:, lanes] = scaled_grad * x_ref[:, lanes].astype(F32)
        dx_ref[:, lanes] = (scaled_grad * step_wide[:, lanes]).astype(BF16)
        db_ref[:, states] = (dbp_ref[:, states] + mm((scaled * ends).astype(BF16), later)).astype(
            BF16
        )
        both = before_rows[lanes].astype(F32) * later.astype(F32)
        carried.append(jnp.sum(both, axis=1, keepdims=True))
    ended = mm(total_ref[...], wide, 1, 1, precision=HIGHEST)
    stepped = mm(g_ref[...], wide, 1, 1, precision=HIGHEST)
    both = jnp.broadcast_to(jnp.concatenate(carried, axis=0), (channels, STATE))
    carried = mm(jnp.ones((8, STATE), F32), mm(wide, both, precision=HIGHEST), 1, 1, HIGHEST)
    carried = carried[:1] * (1.0 / STATE) * jnp.exp(down[tokens - 1 : tokens, :])
    moved = moved_ref[...] - ended
    final = jnp.sum(ended, axis=0, keepdims=True) + carried
    lower = jnp.where(mask, 1.0, 0.0).astype(F32)
    decay_grad = mm(lower, moved, 0, 0, precision=HIGHEST) + final
    dstep_ref[...] = (stepped - rate_ref[...] * decay_grad).T

    save(dx_ref, dx_hbm)
    save(db_ref, db_hbm)
    save(dstep_ref, dstep_hbm)

    for d in range(1, n_sp):
        src_span = at.span_back(d)
        block = mix_cols.at[src_span, stripe(t)]
        landed(block, cols_recv.at[src_span, t])
        for i, peer in enumerate(near):
            push(block, block, near_send.at[d, i], cols_recv.at[src_span, t], (me, peer))
    norm_there += norm_ring.advance()
    for d in range(1, n_sp):
        src_span = at.span_back(d)
        for j, owner in enumerate(at.outers()):
            block = mix_cols.at[src_span, stripe(owner)]
            landed(block, cols_recv.at[src_span, owner])
            for i, partner in enumerate(at.partners()):
                push(block, block, fwd_send.at[d, j, i], cols_recv.at[src_span, owner], (me, partner))
    for d in range(1, n_sp):
        src_span = at.span_back(d)
        for partner in at.partners():
            core = lax.rem(partner, at.inner)
            for far in range(at.outer):
                owner = far * at.inner + core
                landed(mix_cols.at[src_span, stripe(owner)], cols_recv.at[src_span, owner])
    proj_ref[...] = jnp.zeros(proj_ref.shape, F32)
    while True:
        for slot in norm_there:
            proj_ref[...] += mm(norm_ring.block(slot)[...], mix_cols[norm_ring.origin(slot)])
        if not norm_ring.more():
            break
        norm_there = norm_ring.advance()
    save(proj_ref, proj_hbm)
    for wait in waits:
        wait()
    for copy in saves:
        copy.wait()


def main_part(stream, own_grad, routes, combine, weights, entering, scan_args, out_weight, n_sp, n_tp):
    tokens, width = own_grad.shape
    model_width, units = weights[0].shape
    capacity = -(-3 * tokens // n_sp)
    capacity = -(-capacity // 16) * 16
    pairs = n_sp * capacity
    x, step, rate, extra, b_rows, c_rows, gate, scale = scan_args
    channels = x.shape[1]
    heads = step.shape[0]
    per, lanes = channels // n_sp, entering.shape[1]
    out_columns = out_weight.shape[1]
    inner = 2 if n_tp % 2 == 0 else 1
    outer = n_tp // inner
    mates, others = max(inner - 1, 1), max(outer - 1, 1)
    near = max(inner + outer - 2, 1)
    blocks = (n_sp, capacity, width)
    states = (n_sp, per, lanes)

    def low(*shape):
        return pltpu.VMEM(shape, BF16)

    def full(*shape):
        return pltpu.VMEM(shape, F32)

    def out(shape, dtype):
        return jax.ShapeDtypeStruct(shape, dtype)

    anywhere = pl.BlockSpec(memory_space=pl.ANY)
    args = (stream, own_grad, routes, combine, *weights, entering, *scan_args, out_weight)
    return pl.pallas_call(
        functools.partial(main_kernel, n_sp, n_tp),
        out_shape=(
            out((model_width, pairs), BF16),
            out((units, model_width), BF16),
            out((pairs, units), BF16),
            out((pairs, units), BF16),
            out((channels, out_columns), F32),
            out(x.shape, BF16),
            out(step.shape, F32),
            out(b_rows.shape, BF16),
            out(c_rows.shape, BF16),
            out(x.shape, BF16),
        ),
        in_specs=whole(4) + [anywhere] * 3 + whole(len(args) - 7),
        out_specs=tuple([anywhere] * 10),
        scratch_shapes=[
            full(channels, out_columns),
            low(*x.shape),
            full(*step.shape),
            low(*b_rows.shape),
            low(*c_rows.shape),
            low(*x.shape),
            low(n_sp, capacity, model_width),
            low(n_sp, capacity, model_width),
            low(model_width, pairs),
            low(pairs, units),
            low(units, pairs),
            low(pairs, units),
            low(pairs, units),
            low(*blocks),
            low(*blocks),
            low(n_sp, tokens, capacity),
            low(*states),
            low(*states),
            low(n_sp, 1, lanes),
            low(n_sp, 1, lanes),
            DMA((2, n_sp)),
            DMA((2, n_sp, near)),
            DMA((2, n_sp, max((outer - 1) * (inner - 1), 1))),
            DMA((2, n_sp, n_tp)),
            DMA((n_sp,)),
            DMA((n_sp,)),
            DMA((n_sp,)),
            DMA((n_sp,)),
            DMA((10,)),
            low(model_width, units),
            low(model_width, units),
            low(units, model_width),
            full(pairs, units),
            full(pairs, units),
            full(pairs, units),
            low(n_sp, capacity, model_width),
            low(mates, outer, *blocks),
            low(others, *blocks),
            low(others, *blocks),
            low(*blocks),
            low(*blocks),
            low(*states),
            low(*states),
            low(tokens, width),
            low(tokens, model_width),
            low(n_sp, tokens, out_columns),
            low(n_sp, tokens, out_columns),
            low(n_sp, channels, out_columns),
            low(channels, tokens),
            low(n_sp, channels, tokens),
            full(tokens, channels),
            full(tokens, channels),
            full(tokens, channels),
            full(tokens, channels),
            full(tokens, channels),
            full(tokens, channels),
            full(tokens, channels),
            full(*b_rows.shape),
            full(tokens, heads),
            low(*states),
            low(*states),
            low(*states),
            low(*states),
            DMA((3,)),
            DMA((mates, outer, n_sp)),
            DMA((mates, outer, n_sp)),
            DMA((others, n_sp)),
            DMA((others, n_sp)),
            DMA((n_sp,)),
            DMA((n_sp,)),
            DMA((outer, near)),
            DMA((n_tp,)),
            DMA((n_sp,)),
            DMA((n_sp,)),
            DMA((n_sp, 2)),
            DMA((n_sp, 2)),
            DMA((n_sp, 2)),
            DMA((n_sp, 2)),
            DMA((n_sp,)),
            DMA((n_sp,)),
            DMA((n_sp,)),
            DMA((n_sp,)),
            DMA((n_sp,)),
            DMA((n_sp, near)),
            DMA((n_sp, others, mates)),
            DMA((n_sp, n_tp)),
        ],
        compiler_params=pltpu.CompilerParams(
            collective_id=2, has_side_effects=True, vmem_limit_bytes=67_000_000
        ),
        name="main_part",
    )(*args)


def weight_grad_kernel(count, rows_ref, gate_ref, up_ref, *rest):
    ready, (g_out, u_out), out = rest[:count], rest[count : count + 2], rest[count + 2 :]
    g_out[...] = mm(rows_ref[...], gate_ref[...]).astype(BF16)
    u_out[...] = mm(rows_ref[...], up_ref[...]).astype(BF16)
    for source, target in zip(ready, out):
        target[...] = source[...]


def expert_weight_grads(rows_t, gate_grad, up_grad, ready):
    model_width, pairs = rows_t.shape
    units = gate_grad.shape[1]
    tile = 512
    steps = model_width // tile
    fixed = pl.BlockSpec((pairs, units), lambda i: (0, 0))
    tall = pl.BlockSpec((tile, units), lambda i: (i, 0))
    handed = []
    for array in ready:
        if array.shape[0] % (16 * steps):
            handed.append(pl.BlockSpec(array.shape, lambda i: (0, 0)))
        else:
            handed.append(pl.BlockSpec((array.shape[0] // steps, array.shape[1]), lambda i: (i, 0)))
    return pl.pallas_call(
        functools.partial(weight_grad_kernel, len(ready)),
        grid=(steps,),
        out_shape=(
            jax.ShapeDtypeStruct((model_width, units), BF16),
            jax.ShapeDtypeStruct((model_width, units), BF16),
            *(jax.ShapeDtypeStruct(array.shape, array.dtype) for array in ready),
        ),
        in_specs=[
            pl.BlockSpec((tile, pairs), lambda i: (i, 0)),
            fixed,
            fixed,
            *handed,
        ],
        out_specs=(tall, tall, *handed),
        name="expert_weight_grads",
    )(rows_t, gate_grad, up_grad, *ready)


def body(
    mixer_output_stream,
    layer_output_gradient,
    routes,
    expert_combine_weight,
    expert_gate_weight,
    expert_up_weight,
    expert_down_weight,
    head_mixer_input,
    head_step_size,
    head_decay_rate,
    extra_log_decay,
    state_entering_span,
    state_input_vectors,
    state_readout_vectors,
    gate_preactivation,
    group_norm_scale,
    mixer_output_weight,
):
    n_sp, n_tp = lax.axis_size("sp"), lax.axis_size("tp")
    rows_t, grad_d, gate_grad, up_grad, *ready = main_part(
        mixer_output_stream,
        layer_output_gradient,
        routes.T,
        expert_combine_weight.T,
        (expert_gate_weight[0], expert_up_weight[0], expert_down_weight[0]),
        state_entering_span.reshape(-1, STATE),
        (
            head_mixer_input,
            head_step_size.T,
            head_decay_rate[None, :],
            extra_log_decay.T,
            state_input_vectors,
            state_readout_vectors,
            gate_preactivation,
            group_norm_scale[None, :],
        ),
        mixer_output_weight,
        n_sp,
        n_tp,
    )
    grad_g, grad_u, grad_d, proj_grad, input_grad, step_grad, b_grad, c_grad, gate_grad_in = (
        expert_weight_grads(rows_t, gate_grad, up_grad, [grad_d, *ready])
    )
    return (
        grad_g[None],
        grad_u[None],
        grad_d[None],
        proj_grad,
        input_grad,
        step_grad.T,
        b_grad,
        c_grad,
        gate_grad_in,
    )


def solution(mesh):
    return jax.shard_map(
        body,
        mesh=mesh,
        in_specs=(
            P("sp", "tp"),
            P("sp", "tp"),
            P("sp", None),
            P("sp", None),
            P("sp", None, "tp"),
            P("sp", None, "tp"),
            P("sp", "tp", None),
            P("sp", "tp"),
            P("sp", "tp"),
            P("tp"),
            P("sp", "tp"),
            P("tp", None, None),
            P("sp", "tp"),
            P("sp", "tp"),
            P("sp", "tp"),
            P("tp"),
            P("tp", "sp"),
        ),
        out_specs=(
            P("sp", None, "tp"),
            P("sp", None, "tp"),
            P("sp", "tp", None),
            P("tp", "sp"),
            P("sp", "tp"),
            P("sp", "tp"),
            P("sp", "tp"),
            P("sp", "tp"),
            P("sp", "tp"),
        ),
        check_vma=False,
    )
```
